512 devices in a mesh: ep: 32 (over z, x), tp: 16 (over y, core).
Axes of the slice: x: 4, y: 8, z: 8, core: 2. Of those that a mesh axis runs over, the one named last changes fastest.
Arguments:
- queries: bfloat16 [4096, 512], P('ep'), may hold values from -6 to 6
- key_vectors: bfloat16 [4096, 512], P('ep'), may hold values from -6 to 6
- values: bfloat16 [4096, 1024], P('ep', 'tp'), may hold values from -6 to 6
- out_gate: bfloat16 [4096, 1024], P('ep', 'tp'), may hold values from -6 to 6
- input_gate: float32 [4096, 2], P('ep'), may hold values from -8 to 130
- forget_gate: float32 [4096, 2], P('ep'), may hold values from -2 to 16
- mix_weight: bfloat16 [1024, 2048], P('tp'), may hold values from -0.1875 to 0.1875
- expert_input: bfloat16 [8192, 2048], P('ep'), may hold values from -6 to 6
- norm_gain: float32 [2048], replicated, may hold values from 0.1 to 1.9
- route_ids: int32 [8192, 4], P('ep'), may hold values from 0 to 63, all different within a row; in each aligned block of 256 rows (0 to 255, 256 to 511, ...) at most 32 rows name the same one
- route_weights: float32 [8192, 4], P('ep'), may hold values from 0.2 to 1.2
- expert_gate: bfloat16 [512, 2048, 128], P(('ep', 'tp')), may hold values from -0.125 to 0.125
- expert_up: bfloat16 [512, 2048, 128], P(('ep', 'tp')), may hold values from -0.125 to 0.125
- expert_down: bfloat16 [512, 128, 2048], P(('ep', 'tp')), may hold values from -0.1875 to 0.1875
- shared_gate: bfloat16 [2048, 512], P(None, 'tp'), may hold values from -0.125 to 0.125
- shared_up: bfloat16 [2048, 512], P(None, 'tp'), may hold values from -0.125 to 0.125
- shared_down: bfloat16 [512, 2048], P('tp'), may hold values from -0.25 to 0.25
Outputs:
- mixer_out: bfloat16 [4096, 2048], P('ep')
- expert_out: bfloat16 [8192, 2048], P('ep')
The draws below stay inside these ranges and needn't reach their ends.
Inputs may be any that keep to these rules, and one draw needn't show every extreme that they name: `route_ids`: each row names 4 different experts. In each aligned block of 256 rows (the rows of one index of ep) no expert is named by more than 32 rows, and in some block one expert is named by exactly 32 rows.
All inputs are finite; a program needn't handle non-finite values.
Results may differ from the reference program's by a relative error of at most 0.01575.
Values may be sent and summed in bfloat16 or wider, within the bound.
No kernel may reach another device: no remote copies, remote signals or barrier semaphores. Data moves between devices by JAX's collectives and lax.ppermute only.
A program may use at most 64 MiB of HBM per device.

```python
import math
import jax
import jax.numpy as jnp
import numpy as np
from jax import lax

D = 2048
MEMORY_HEADS = 2
KEY_DIM = 256
VAL_DIM = 512
BLOCK = 128
MOE_DEV = 256
TOPK = 4
FF = 1024
FF_SHARED = 512
MIXER_TOKEN_COUNT = 4096
MOE_TOKENS = 8192
TP_GROUP = 8
FF_DEV = 128
EXPERTS = 64
CAP = 32
VAL_DEV = 64
N_EP = 32
N_TP = 16


def draw_input_gate(key, part):
    random_subkeys = jax.random.split(jax.random.fold_in(key, 23), 1)
    pre_gate = jnp.clip(1.5 * jax.random.normal(random_subkeys[0], (MIXER_TOKEN_COUNT, MEMORY_HEADS), jnp.float32), -7.5, 7.5)
    return pre_gate


def draw_forget_gate(key, part):
    random_subkeys = jax.random.split(jax.random.fold_in(key, 41), 5)
    token_positions = jnp.arange(MIXER_TOKEN_COUNT, dtype=jnp.int32)
    shuffled = jax.random.permutation(random_subkeys[0], MEMORY_HEADS)
    slow_heads = (shuffled < MEMORY_HEADS // 2).astype(jnp.float32)
    slow_rate = 0.5
    baseline_rate = slow_heads * (slow_rate / MIXER_TOKEN_COUNT) + (1.0 - slow_heads) / 40.0
    block_multiplier = jnp.exp(jax.random.uniform(random_subkeys[1], (MIXER_TOKEN_COUNT // BLOCK, MEMORY_HEADS), jnp.float32, -0.69, 0.69))
    block_multiplier = jnp.repeat(block_multiplier, BLOCK, axis=0)
    jitter_amount = jnp.exp(jax.random.uniform(random_subkeys[2], (MIXER_TOKEN_COUNT, MEMORY_HEADS), jnp.float32, -1.1, 1.1))
    spike_position = jax.random.randint(random_subkeys[3], (3, MEMORY_HEADS), 0, MIXER_TOKEN_COUNT)
    spike_flag = jnp.any(token_positions[:, None, None] == spike_position[None, :, :], axis=1)
    spike_magnitude = jnp.log(jax.random.uniform(random_subkeys[4], (MIXER_TOKEN_COUNT, MEMORY_HEADS), jnp.float32, 0.5, 0.8))
    log_retention = -baseline_rate[None, :] * block_multiplier * jitter_amount + jnp.where(spike_flag, spike_magnitude, 0.0)
    return log_retention - jnp.log(-jnp.expm1(log_retention))


def levels(stream_key, dims, shards, least, high):
    def one(dim, shards_of):
        steps = jax.random.uniform(jax.random.fold_in(jax.random.fold_in(stream_key, 6), dim), (shards_of,), jnp.float32, least / len(shards), high / len(shards))
        return jnp.repeat(jnp.exp(steps), dims[dim] // shards_of).reshape((-1,) + (1,) * (len(dims) - dim - 1))

    factor_of = one(*shards[0])
    for cut in shards[1:]:
        factor_of = factor_of * one(*cut)
    return factor_of


def deal_out(stream_key, own, number, rows, count, top, limit, lean):
    order = jax.random.permutation(stream_key, count)
    crowded, ordinary = shares(count, rows * top, limit, lean, True), shares(count, rows * top, limit, lean, False)
    places = jnp.arange(count)

    def named(tallies, rotation):
        used = int((tallies > 0).sum())
        fixed = max(1, used // 4)
        shifted = fixed + (places - fixed + rotation * (used - fixed)) % max(1, count - fixed)
        return jnp.zeros((count,), jnp.int32).at[order[jnp.where(places < fixed, places, shifted)]].set(jnp.asarray(tallies, jnp.int32))

    tallies = jnp.where(number % 4 == 0, named(crowded, number // 4), named(ordinary, number - number // 4 - 1))
    mixed = jax.random.permutation(jax.random.fold_in(own, 3), count)
    donor, sink = mixed[0:count // 2 * 2:2], mixed[1:count // 2 * 2:2]
    margin = jnp.minimum(tallies[donor] - 1, limit - tallies[sink]) // 2
    margin = jnp.where((donor == order[0]) | (sink == order[0]) | (tallies[sink] == 0), 0, jnp.maximum(margin, 0))
    shifted = jax.random.randint(jax.random.fold_in(own, 4), (count // 2,), 0, 1 << 20) % (margin + 1)
    tallies = tallies.at[donor].add(-shifted).at[sink].add(shifted)
    members = jnp.searchsorted(jnp.cumsum(tallies), jnp.arange(rows * top), side="right").astype(jnp.int32)
    grid = members.reshape(top, rows).T
    grid = grid[jax.random.permutation(jax.random.fold_in(own, 1), rows)]
    rotation = jax.random.randint(jax.random.fold_in(own, 2), (rows, 1), 0, top)
    return jnp.take_along_axis(grid, (jnp.arange(top)[None, :] + rotation) % top, axis=1)


def shares(count, total, limit, skew, full):
    weights = [(1 << 20) // math.isqrt(standing ** skew) + 1 for standing in range(1, count + 1)]
    largest = limit if full else min(limit, max(-(-total // count), total * weights[0] // sum(weights)))
    least = 1 if total - largest >= count - 1 else 0
    given, rest = [largest] + [least] * (count - 1), total - largest - least * (count - 1)
    while rest > 0:
        free = [i for i in range(1, count) if given[i] < largest] or [i for i in range(1, count) if given[i] < limit]
        pool, left = sum([weights[i] for i in free]), rest
        for i in free:
            extra = min(limit - given[i], max(1, left * weights[i] // pool), rest)
            given[i] = given[i] + extra
            rest = rest - extra
    return np.array(given)


def centred(rng, shape, width, reach, shards=(), held_as=jnp.bfloat16):
    entries = width * jax.random.normal(rng, shape, jnp.float32)
    if shards:
        entries = entries * levels(rng, shape, shards, -0.22, 0.18)
    return jnp.clip(entries, -reach, reach).astype(held_as)


def setup_inputs(seed: int = 0) -> dict:
    keys = jax.random.split(jax.random.key(seed), 18)
    queries = centred(keys[0], (MIXER_TOKEN_COUNT, MEMORY_HEADS * KEY_DIM), 1.0, 6.0, ((0, 32),))
    key_vectors = centred(keys[1], (MIXER_TOKEN_COUNT, MEMORY_HEADS * KEY_DIM), 1.0, 6.0, ((0, 32),))
    values = centred(keys[2], (MIXER_TOKEN_COUNT, MEMORY_HEADS * VAL_DIM), 1.0, 6.0, ((0, 32), (1, 16)))
    out_gate = centred(keys[3], (MIXER_TOKEN_COUNT, MEMORY_HEADS * VAL_DIM), 1.0, 6.0, ((0, 32), (1, 16)))
    input_gate = draw_input_gate(jax.random.fold_in(keys[17], 71), 0)
    forget_gate = draw_forget_gate(jax.random.fold_in(keys[17], 71), 0)
    mix_weight = centred(keys[6], (MEMORY_HEADS * VAL_DIM, D), (MEMORY_HEADS * VAL_DIM) ** -0.5, 0.1875, ((0, 16),))
    expert_input = centred(keys[7], (MOE_TOKENS, D), 1.0, 6.0, ((0, 32),))
    norm_gain = jnp.clip(1.0 + 0.18 * jax.random.normal(keys[8], (D,), jnp.float32), 0.1, 1.9)
    route_ids_keys = jax.random.split(jax.random.fold_in(keys[9], 1), MOE_TOKENS // MOE_DEV)
    route_ids_turns = jax.random.permutation(jax.random.fold_in(keys[9], 3), MOE_TOKENS // MOE_DEV)
    route_ids = jax.vmap(lambda own, number: deal_out(jax.random.fold_in(keys[9], 2), own, number, MOE_DEV, EXPERTS, TOPK, CAP, 2))(route_ids_keys, route_ids_turns).reshape((MOE_TOKENS, TOPK))
    route_weights = jnp.clip(0.2 + 1 * jax.random.uniform(keys[10], (MOE_TOKENS, TOPK), jnp.float32) ** levels(keys[10], (MOE_TOKENS, TOPK), ((0, 32),), -0.2, 0.2), 0.2, 1.2)
    expert_gate = centred(keys[11], (EXPERTS * TP_GROUP, D, FF_DEV), D ** -0.5, 0.125, ((0, 512),))
    expert_up = centred(keys[12], (EXPERTS * TP_GROUP, D, FF_DEV), D ** -0.5, 0.125, ((0, 512),))
    expert_down = centred(keys[13], (EXPERTS * TP_GROUP, FF_DEV, D), FF ** -0.5, 0.1875, ((0, 512),))
    shared_gate = centred(keys[14], (D, FF_SHARED), D ** -0.5, 0.125, ((1, 16),))
    shared_up = centred(keys[15], (D, FF_SHARED), D ** -0.5, 0.125, ((1, 16),))
    shared_down = centred(keys[16], (FF_SHARED, D), FF_SHARED ** -0.5, 0.25, ((0, 16),))
    return dict(queries=queries, key_vectors=key_vectors, values=values, out_gate=out_gate, input_gate=input_gate, forget_gate=forget_gate, mix_weight=mix_weight, expert_input=expert_input, norm_gain=norm_gain, route_ids=route_ids, route_weights=route_weights, expert_gate=expert_gate, expert_up=expert_up, expert_down=expert_down, shared_gate=shared_gate, shared_up=shared_up, shared_down=shared_down)


epsilon = 1e-06
den_floor = 4.0

def mixer_part(queries, key_vectors, values, out_gate, input_gate, forget_gate, mix_weight):
    length = queries.shape[0]
    blocks = length // BLOCK
    factor = KEY_DIM ** (-0.5)
    causal = jnp.tril(jnp.ones((BLOCK, BLOCK), dtype=bool))

    def by_head(matrix, columns):
        return matrix.reshape(blocks, BLOCK, MEMORY_HEADS, columns).transpose(0, 2, 1, 3)
    query_blocks = by_head(queries, KEY_DIM)
    key_blocks = by_head(key_vectors, KEY_DIM)
    value_blocks = by_head(values, VAL_DIM)
    input_blocks = input_gate.reshape(blocks, BLOCK, MEMORY_HEADS).transpose(0, 2, 1)
    forget_blocks = jax.nn.log_sigmoid(forget_gate).reshape(blocks, BLOCK, MEMORY_HEADS).transpose(0, 2, 1)

    def block_step(carry_in, inputs):
        memory, normalizer, running = carry_in
        query_block, key_block, value_block, input_block, forget_block = inputs
        cumulative = jnp.cumsum(forget_block, axis=-1)
        carried = cumulative + running[:, None]
        log_weight = cumulative[:, :, None] - cumulative[:, None, :] + input_block[:, None, :]
        log_weight = jnp.where(causal, log_weight, -jnp.inf)
        stabilizer = jnp.maximum(carried, lax.optimization_barrier(jnp.max(log_weight, axis=-1)))
        within = jnp.exp(log_weight - stabilizer[:, :, None])
        across = jnp.exp(carried - stabilizer)
        query_wide = query_block.astype(jnp.float32)
        key_wide = key_block.astype(jnp.float32)
        value_wide = value_block.astype(jnp.float32)
        scores = jnp.einsum('htd,hsd->hts', query_wide, key_wide) * factor
        weights = scores * within
        weights_low = lax.optimization_barrier(weights.astype(jnp.bfloat16)).astype(jnp.float32)
        scaled = query_wide * factor
        numerator = across[:, :, None] * jnp.einsum('htd,hdv->htv', scaled, memory, precision=lax.Precision.HIGHEST)
        numerator = numerator + jnp.einsum('hts,hsv->htv', weights_low, value_wide)
        denominator = across * jnp.einsum('htd,hd->ht', scaled, normalizer, precision=lax.Precision.HIGHEST)
        denominator = denominator + lax.optimization_barrier(jnp.sum(weights, axis=-1))
        hidden = numerator / jnp.maximum(jnp.abs(denominator), den_floor)[:, :, None]
        block_total = cumulative[:, -1]
        log_retention = block_total[:, None] - cumulative + input_block
        running_next = jnp.maximum(block_total + running, lax.optimization_barrier(jnp.max(log_retention, axis=-1)))
        carry_decay = jnp.exp(block_total + running - running_next)
        weighted_keys = key_wide * jnp.exp(log_retention - running_next[:, None])[:, :, None]
        memory = carry_decay[:, None, None] * memory + jnp.einsum('hsd,hsv->hdv', weighted_keys, value_wide, precision=lax.Precision.HIGHEST)
        normalizer = carry_decay[:, None] * normalizer + lax.optimization_barrier(jnp.sum(weighted_keys, axis=1))
        return ((memory, normalizer, running_next), hidden)
    initial = (jnp.zeros((MEMORY_HEADS, KEY_DIM, VAL_DIM), jnp.float32), jnp.zeros((MEMORY_HEADS, KEY_DIM), jnp.float32), jnp.zeros((MEMORY_HEADS,), jnp.float32))
    _, hidden = lax.scan(block_step, initial, (query_blocks, key_blocks, value_blocks, input_blocks, forget_blocks))
    hidden = hidden.transpose(0, 2, 1, 3).reshape(length, MEMORY_HEADS * VAL_DIM)
    gated_rows = (hidden * jax.nn.sigmoid(out_gate.astype(jnp.float32))).astype(jnp.bfloat16)

    def add_group(summed, group_index):
        offset = (group_index * VAL_DEV).astype(jnp.int32)
        partial_value = jnp.dot(lax.dynamic_slice_in_dim(gated_rows, offset, VAL_DEV, 1), lax.dynamic_slice_in_dim(mix_weight, offset, VAL_DEV, 0), preferred_element_type=jnp.float32)
        return (summed + lax.optimization_barrier(partial_value.astype(jnp.bfloat16)).astype(jnp.float32), None)
    summed, _ = lax.scan(add_group, jnp.zeros((length, D), jnp.float32), jnp.arange(N_TP, dtype=jnp.int32))
    return summed.astype(jnp.bfloat16)

def expert_part(expert_input, norm_gain, route_ids, route_weights, expert_gate, expert_up, expert_down, shared_gate, shared_up, shared_down):
    rows_wide = expert_input.astype(jnp.float32)
    normed = (rows_wide * lax.rsqrt(lax.optimization_barrier(jnp.mean(rows_wide * rows_wide, axis=-1, keepdims=True)) + epsilon) * norm_gain).astype(jnp.bfloat16)
    chosen = route_ids.reshape(N_EP, MOE_DEV * TOPK)
    onehot = (chosen[:, :, None] == jnp.arange(EXPERTS, dtype=jnp.int32)[None, None, :]).astype(jnp.int32)
    earlier = jnp.cumsum(onehot, axis=1) - onehot
    slot_rank = lax.optimization_barrier(jnp.sum(earlier * onehot, axis=2))
    slot_index = (jnp.arange(N_EP, dtype=jnp.int32)[:, None] * CAP + slot_rank).reshape(-1)
    expert_of = route_ids.reshape(-1)
    token_of = jnp.arange(MOE_TOKENS * TOPK, dtype=jnp.int32) // TOPK
    slot_token = jnp.zeros((EXPERTS, N_EP * CAP), jnp.int32).at[expert_of, slot_index].set(token_of)
    slot_weight = jnp.zeros((EXPERTS, N_EP * CAP), jnp.float32).at[expert_of, slot_index].set(route_weights.reshape(-1))

    def one_expert(routed, expert_index):
        tokens_here = slot_token[expert_index]
        weight_here = slot_weight[expert_index]
        picked = normed[tokens_here].astype(jnp.float32)
        rows_base = (expert_index * TP_GROUP).astype(jnp.int32)
        gate_w = lax.dynamic_slice_in_dim(expert_gate, rows_base, TP_GROUP, 0).astype(jnp.float32)
        up_w = lax.dynamic_slice_in_dim(expert_up, rows_base, TP_GROUP, 0).astype(jnp.float32)
        down_w = lax.dynamic_slice_in_dim(expert_down, rows_base, TP_GROUP, 0).astype(jnp.float32)
        gate_val = jnp.einsum('rd,gdf->rgf', picked, gate_w)
        up_val = jnp.einsum('rd,gdf->rgf', picked, up_w)
        hidden = lax.optimization_barrier((jax.nn.silu(gate_val) * up_val).astype(jnp.bfloat16)).astype(jnp.float32)
        partials = jnp.einsum('rgf,gfd->rgd', hidden, down_w)
        partials = lax.optimization_barrier(partials.astype(jnp.bfloat16)).astype(jnp.float32)
        result = lax.optimization_barrier(jnp.sum(partials, axis=1)) * weight_here[:, None]
        return (routed.at[tokens_here].add(result), None)
    routed, _ = lax.scan(one_expert, jnp.zeros((MOE_TOKENS, D), jnp.float32), jnp.arange(EXPERTS, dtype=jnp.int32))
    shared_gate_val = jnp.dot(normed, shared_gate, preferred_element_type=jnp.float32)
    shared_up_val = jnp.dot(normed, shared_up, preferred_element_type=jnp.float32)
    shared_act = (jax.nn.silu(shared_gate_val) * shared_up_val).astype(jnp.bfloat16)
    shared_rows = jnp.dot(shared_act, shared_down, preferred_element_type=jnp.float32)
    return (routed + shared_rows).astype(jnp.bfloat16)

def reference(queries, key_vectors, values, out_gate, input_gate, forget_gate, mix_weight, expert_input, norm_gain, route_ids, route_weights, expert_gate, expert_up, expert_down, shared_gate, shared_up, shared_down):
    mixer_out = mixer_part(queries, key_vectors, values, out_gate, input_gate, forget_gate, mix_weight)
    expert_out = expert_part(expert_input, norm_gain, route_ids, route_weights, expert_gate, expert_up, expert_down, shared_gate, shared_up, shared_down)
    return (mixer_out, expert_out)
```

```python
import functools

import jax
import jax.numpy as jnp
from jax import lax
from jax.experimental import pallas as pl
from jax.experimental.pallas import tpu as pltpu
from jax.sharding import Mesh
from jax.sharding import PartitionSpec as P

D = 2048
KEY_DIM = 256
BLOCK = 128
N_EP = 32
SLOTS = 8
TOKENS = 256
EP = ("z", "x")
EP_TP = ("z", "x", "y", "c")
TP = ("y", "c")
bf16 = jnp.bfloat16
f32 = jnp.float32
epsilon = 1e-06
lowest = -1e30
den_floor = 4.0
HIGHEST = lax.Precision.HIGHEST

VMEM = pl.BlockSpec(memory_space=pltpu.VMEM)
SMEM = pl.BlockSpec(memory_space=pltpu.SMEM)
NT = (((1,), (1,)), ((), ()))
TN = (((0,), (0,)), ((), ()))


def call(body, place, arrays, outs, flops):
    return pl.pallas_call(
        body,
        out_shape=outs,
        in_specs=[SMEM] + [VMEM] * len(arrays),
        out_specs=[VMEM] * len(outs),
        compiler_params=pltpu.CompilerParams(vmem_limit_bytes=48 << 20),
        cost_estimate=pl.CostEstimate(flops=flops, bytes_accessed=1 << 20, transcendentals=0),
    )(place, *arrays)


def shape(dims, dtype):
    return jax.ShapeDtypeStruct(dims, dtype)


def iota(dims, dim):
    return lax.broadcasted_iota(jnp.int32, dims, dim)


def route_kernel(place, x, gain, ids, weights, send, normed, w_high, w_low):
    team, part = place[0], place[1]
    rows = x[...].astype(f32)
    scale = lax.rsqrt(jnp.mean(rows * rows, axis=-1, keepdims=True) + epsilon)
    normal = (rows * scale * gain[...]).astype(bf16)
    normed[...] = normal
    expert = iota((N_EP, TOKENS), 0) * 2 + team
    named = jnp.zeros((N_EP, TOKENS), f32)
    weight = jnp.zeros((N_EP, TOKENS), f32)
    for k in range(4):
        hit = ids[k : k + 1, :] == expert
        named = named + jnp.where(hit, 1.0, 0.0)
        weight = weight + jnp.where(hit, weights[k : k + 1, :], 0.0)
    before = jnp.where(iota((TOKENS, TOKENS), 0) < iota((TOKENS, TOKENS), 1), 1.0, 0.0).astype(bf16)
    rank = jnp.dot(named.astype(bf16), before, preferred_element_type=f32)
    rank = jnp.where(named > 0.0, rank, -1.0)
    slots = N_EP * SLOTS
    spread = jnp.where(iota((slots, N_EP), 0) // SLOTS == iota((slots, N_EP), 1), 1.0, 0.0)
    rank = jnp.dot(spread.astype(bf16), rank.astype(bf16), preferred_element_type=f32)
    weight = jnp.dot(spread, weight, preferred_element_type=f32, precision=HIGHEST)
    slot = (iota((slots, TOKENS), 0) % SLOTS + part * SLOTS).astype(f32)
    chosen = rank == slot
    pick = jnp.where(chosen, 1.0, 0.0).astype(bf16)
    send[...] = jnp.dot(pick, normal, preferred_element_type=f32).astype(bf16)
    weight = jnp.where(chosen, weight, 0.0)
    high = weight.astype(bf16)
    w_high[...] = high
    w_low[...] = (weight - high.astype(f32)).astype(bf16)


def pack_kernel(place, gate, up, down, packed):
    packed[0:D, :] = gate[...]
    packed[D : 2 * D, :] = up[...]
    for k in range(16):
        packed[2 * D + 128 * k : 2 * D + 128 * (k + 1), :] = down[:, 128 * k : 128 * (k + 1)]


def expert_kernel(place, x, own, core, near, far, out):
    rows = x[...]
    acts = []
    packs = (own, core, near, far)
    for pack in packs:
        gate = jnp.dot(rows, pack[0:D, :], preferred_element_type=f32)
        up = jnp.dot(rows, pack[D : 2 * D, :], preferred_element_type=f32)
        acts.append((gate / (1.0 + jnp.exp(-gate)) * up).astype(bf16))
    for k in range(16):
        part = slice(2 * D + 128 * k, 2 * D + 128 * (k + 1))
        total = jnp.zeros((TOKENS, 128), f32)
        for act, pack in zip(acts, packs):
            total = total + jnp.dot(act, pack[part, :], preferred_element_type=f32)
        out[:, 128 * k : 128 * (k + 1)] = total.astype(bf16)


def shared_kernel(place, x, gate, up, act):
    rows = x[...]
    gated = lax.dot_general(rows, gate[...], NT, preferred_element_type=f32)
    lifted = lax.dot_general(rows, up[...], NT, preferred_element_type=f32)
    act[...] = (gated / (1.0 + jnp.exp(-gated)) * lifted).astype(bf16)


def combine_kernel(place, back, w_high, w_low, act, down, keep, give, total):
    core = place[2]
    rows = back[...]
    total[...] = (
        lax.dot_general(w_high[...], rows, TN, preferred_element_type=f32)
        + lax.dot_general(w_low[...], rows, TN, preferred_element_type=f32)
        + jnp.dot(act[...], down[...], preferred_element_type=f32)
    )
    half = TOKENS // 2
    keep[...] = total[pl.ds(pl.multiple_of(core * half, half), half), :]
    give[...] = total[pl.ds(pl.multiple_of((1 - core) * half, half), half), :].astype(bf16)


def gates(place, input_gate, forget_gate):
    first = place[0] == 0
    given = jnp.where(first, input_gate[0:1, :], input_gate[1:2, :])
    forget = jnp.where(first, forget_gate[0:1, :], forget_gate[1:2, :])
    small = jnp.exp(-jnp.abs(forget))
    tail = jnp.where(small < 1e-4, small - 0.5 * small * small, jnp.log(1.0 + small))
    log_forget = jnp.minimum(forget, 0.0) - tail
    upto = jnp.where(iota((BLOCK, BLOCK), 0) <= iota((BLOCK, BLOCK), 1), 1.0, 0.0)
    cumulative = jnp.dot(
        jnp.broadcast_to(log_forget, (8, BLOCK)), upto, preferred_element_type=f32, precision=HIGHEST
    )[0:1, :]
    return given, cumulative


def state_kernel(place, keys, values, input_gate, forget_gate, out):
    given, cumulative = gates(place, input_gate, forget_gate)
    block_total = cumulative[:, BLOCK - 1 : BLOCK]
    log_keep = block_total - cumulative + given
    running = jnp.max(log_keep, axis=1, keepdims=True)
    kept = jnp.exp(log_keep - running)
    key = keys[:, pl.ds(pl.multiple_of(place[0] * KEY_DIM, KEY_DIM), KEY_DIM)].astype(f32)
    memory = jnp.dot(
        values[...].astype(f32) * kept, key, preferred_element_type=f32, precision=HIGHEST
    )
    normalizer = jnp.dot(
        jnp.broadcast_to(kept, (8, BLOCK)), key, preferred_element_type=f32, precision=HIGHEST
    )
    out[:, 0, :] = memory[0:32, 0:128]
    out[:, 1, :] = memory[0:32, 128:256]
    out[:, 2, :] = memory[32:64, 0:128]
    out[:, 3, :] = memory[32:64, 128:256]
    out[:, 4, :] = jnp.broadcast_to(normalizer[0:1, 0:128], (N_EP, 128))
    out[:, 5, :] = jnp.broadcast_to(normalizer[0:1, 128:256], (N_EP, 128))
    out[:, 6, :] = jnp.broadcast_to(block_total, (N_EP, 128))
    out[:, 7, :] = jnp.broadcast_to(running, (N_EP, 128))


def prefix_kernel(place, states, out):
    totals = jnp.broadcast_to(states[:, 6, :][None], (4, N_EP, 128)).reshape(128, 128).T[0:N_EP, 0:N_EP]
    peaks = jnp.broadcast_to(states[:, 7, :][None], (4, N_EP, 128)).reshape(128, 128).T[0:N_EP, 0:N_EP]
    row, column = iota((N_EP, N_EP), 0), iota((N_EP, N_EP), 1)
    earlier = column < row
    passed = jnp.where(earlier, totals, 0.0)
    later = jnp.where(row > column, 1.0, 0.0)
    between = jnp.dot(passed, later, preferred_element_type=f32, precision=HIGHEST)
    reach = jnp.where(earlier, peaks + between, lowest)
    running = jnp.maximum(
        jnp.sum(passed, axis=1, keepdims=True), jnp.max(reach, axis=1, keepdims=True)
    )
    share = jnp.where(earlier, jnp.exp(reach - running), 0.0)
    for k in range(6):
        out[:, k, :] = jnp.dot(share, states[:, k, :], preferred_element_type=f32, precision=HIGHEST)
    out[:, 6, :] = jnp.broadcast_to(running, (N_EP, 128))
    out[:, 7, :] = jnp.zeros((N_EP, 128), f32)


def memory_kernel(
    place, states, queries, keys, values, out_gate, input_gate, forget_gate, mix, keep, give, total
):
    core = place[2]
    given, cumulative = gates(place, input_gate, forget_gate)
    at = pl.ds(pl.multiple_of(place[0] * KEY_DIM, KEY_DIM), KEY_DIM)
    query, key = queries[:, at], keys[:, at]
    factor = KEY_DIM ** (-0.5)
    carried = cumulative + states[0, 6:7, :]
    source = jnp.broadcast_to(given - cumulative, (BLOCK, BLOCK)).T
    allowed = iota((BLOCK, BLOCK), 0) <= iota((BLOCK, BLOCK), 1)
    log_weight = jnp.where(allowed, cumulative + source, lowest)
    stabilizer = jnp.maximum(carried, jnp.max(log_weight, axis=0, keepdims=True))
    within = jnp.exp(log_weight - stabilizer)
    across = jnp.exp(carried - stabilizer)
    scores = lax.dot_general(key, query, NT, preferred_element_type=f32) * factor
    weights = scores * within
    scaled = query.astype(f32) * factor

    def read(first, second):
        return lax.dot_general(
            first, scaled[:, 0:128], NT, preferred_element_type=f32, precision=HIGHEST
        ) + lax.dot_general(
            second, scaled[:, 128:256], NT, preferred_element_type=f32, precision=HIGHEST
        )

    numerator = jnp.concatenate(
        [read(states[:, 0, :], states[:, 1, :]), read(states[:, 2, :], states[:, 3, :])], axis=0
    )
    numerator = across * numerator + jnp.dot(
        values[...], weights.astype(bf16), preferred_element_type=f32
    )
    normalizer = read(
        jnp.broadcast_to(states[0, 4:5, :], (8, 128)), jnp.broadcast_to(states[0, 5:6, :], (8, 128))
    )
    denominator = across * normalizer[0:1, :] + jnp.sum(weights, axis=0, keepdims=True)
    hidden = numerator / jnp.maximum(jnp.abs(denominator), den_floor)
    gated = (hidden / (1.0 + jnp.exp(-out_gate[...].astype(f32)))).astype(bf16)
    total[...] = lax.dot_general(gated, mix[...], TN, preferred_element_type=f32)
    half = BLOCK // 2
    keep[...] = total[pl.ds(pl.multiple_of(core * half, half), half), :]
    give[...] = total[pl.ds(pl.multiple_of((1 - core) * half, half), half), :].astype(bf16)


def exchange(array, axis):
    return lax.all_to_all(array, axis, split_axis=0, concat_axis=0, tiled=True)


def swap(array):
    return lax.ppermute(array, "c", [(0, 1), (1, 0)])


def reach_over(array):
    return lax.ppermute(array, "y", [(k, k ^ 1) for k in range(8)])


def with_scratch(body, place, arrays, outs, flops, rows):
    return pl.pallas_call(
        body,
        out_shape=outs,
        in_specs=[SMEM] + [VMEM] * len(arrays),
        out_specs=[VMEM] * len(outs),
        scratch_shapes=[pltpu.VMEM((rows, D), f32)],
        compiler_params=pltpu.CompilerParams(vmem_limit_bytes=48 << 20),
        cost_estimate=pl.CostEstimate(flops=flops, bytes_accessed=1 << 20, transcendentals=0),
    )(place, *arrays)


def finish(keep, give, core):
    rows = keep.shape[0] // 8
    half = (keep + swap(give).astype(f32)).astype(bf16).reshape(8, rows, D)
    piece = exchange(half, "y").astype(f32).sum(axis=0).astype(bf16)
    mine = exchange(jnp.broadcast_to(piece[None], (8, rows, D)), "y").reshape(8 * rows, D)
    other = swap(mine)
    first = core == 0
    return jnp.concatenate([jnp.where(first, mine, other), jnp.where(first, other, mine)], axis=0)


def shards(
    queries,
    key_vectors,
    values,
    out_gate,
    input_gate,
    forget_gate,
    mix_weight,
    expert_input,
    norm_gain,
    route_ids,
    route_weights,
    expert_gate,
    expert_up,
    expert_down,
    shared_gate,
    shared_up,
    shared_down,
):
    y, core = lax.axis_index("y"), lax.axis_index("c")
    place = jnp.stack([y // 4, (y % 2) * 2 + core, core]).astype(jnp.int32)
    (own,) = call(
        pack_kernel,
        place,
        (expert_gate[0], expert_up[0], expert_down[0]),
        [shape((3 * D, 128), bf16)],
        1 << 20,
    )
    near = reach_over(own)
    beside = swap(own)
    far = swap(near)
    values_t, out_gate_t = values.T, out_gate.T
    input_t, forget_t = input_gate.T, forget_gate.T
    (states,) = call(
        state_kernel,
        place,
        (key_vectors, values_t, input_t, forget_t),
        [shape((N_EP, 8, 128), f32)],
        1 << 20,
    )
    states = exchange(states, EP)
    slots = N_EP * SLOTS
    send, normed, w_high, w_low = call(
        route_kernel,
        place,
        (expert_input, norm_gain[None, :], route_ids.T, route_weights.T),
        [
            shape((slots, D), bf16),
            shape((TOKENS, D), bf16),
            shape((slots, TOKENS), bf16),
            shape((slots, TOKENS), bf16),
        ],
        1 << 28,
    )
    arrived = exchange(send.reshape(N_EP, SLOTS, D), EP).reshape(slots, D)
    (states,) = call(prefix_kernel, place, (states,), [shape((N_EP, 8, 128), f32)], 1 << 20)
    states = exchange(states, EP)
    (act,) = call(
        shared_kernel, place, (normed, shared_gate.T, shared_up.T), [shape((TOKENS, 32), bf16)], 1 << 26
    )
    (results,) = call(
        expert_kernel, place, (arrived, own, beside, near, far), [shape((slots, D), bf16)], 1 << 31
    )
    back = exchange(results.reshape(N_EP, SLOTS, D), EP).reshape(slots, D)
    mixer_keep, mixer_give = with_scratch(
        memory_kernel,
        place,
        (
            states,
            queries,
            key_vectors,
            values_t,
            out_gate_t,
            input_t,
            forget_t,
            mix_weight,
        ),
        [shape((BLOCK // 2, D), f32), shape((BLOCK // 2, D), bf16)],
        1 << 26,
        BLOCK,
    )
    mixer_out = finish(mixer_keep, mixer_give, core)
    keep, give = with_scratch(
        combine_kernel,
        place,
        (back, w_high, w_low, act, shared_down),
        [shape((TOKENS // 2, D), f32), shape((TOKENS // 2, D), bf16)],
        1 << 28,
        TOKENS,
    )
    expert_out = finish(keep, give, core)
    return (mixer_out, expert_out)


def solution(mesh):
    finer = Mesh(mesh.devices.reshape(8, 4, 8, 2), EP_TP)
    placed = (
        P(EP, None),
        P(EP, None),
        P(EP, TP),
        P(EP, TP),
        P(EP, None),
        P(EP, None),
        P(TP, None),
        P(EP, None),
        P(),
        P(EP, None),
        P(EP, None),
        P(EP_TP, None, None),
        P(EP_TP, None, None),
        P(EP_TP, None, None),
        P(None, TP),
        P(None, TP),
        P(TP, None),
    )
    return jax.shard_map(
        shards, mesh=finer, in_specs=placed, out_specs=(P(EP, None), P(EP, None)), check_vma=False
    )
```

```python
import jax
import jax.numpy as jnp
from jax import lax
from jax.experimental import pallas as pl
from jax.experimental.pallas import tpu as pltpu
from jax.sharding import Mesh
from jax.sharding import PartitionSpec as P

D = 2048
WIDE = D + 128
KEY_DIM = 256
BLOCK = 128
N_EP = 32
N_Y = 8
SLOTS = 8
TOKENS = 256
ROWS = N_EP * SLOTS
E_ROWS = TOKENS // 16
M_ROWS = BLOCK // 16
PIECE = E_ROWS + M_ROWS
EP = ("z", "x")
EP_TP = ("z", "x", "y", "c")
TP = ("y", "c")
bf16 = jnp.bfloat16
f32 = jnp.float32
epsilon = 1e-06
lowest = -1e30
den_floor = 4.0
HIGHEST = lax.Precision.HIGHEST

VMEM = pl.BlockSpec(memory_space=pltpu.VMEM)
HBM = pl.BlockSpec(memory_space=pltpu.HBM)
NT = (((1,), (1,)), ((), ()))
TN = (((0,), (0,)), ((), ()))


def call(body, arrays, ins, outs, spaces, scratch, flops, limit=16):
    return pl.pallas_call(
        body,
        out_shape=outs,
        in_specs=ins,
        out_specs=spaces,
        scratch_shapes=scratch,
        compiler_params=pltpu.CompilerParams(vmem_limit_bytes=limit << 20),
        cost_estimate=pl.CostEstimate(flops=flops, bytes_accessed=1 << 20, transcendentals=0),
    )(*arrays)


def shape(dims, dtype):
    return jax.ShapeDtypeStruct(dims, dtype)


def iota(dims, dim):
    return lax.broadcasted_iota(jnp.int32, dims, dim)


def split_scalar(value):
    high = value.astype(bf16).astype(f32)
    middle = (value - high).astype(bf16).astype(f32)
    lane = iota((N_EP, 128), 1)
    return jnp.where(
        lane == 0,
        high,
        jnp.where(lane == 1, middle, jnp.where(lane == 2, value - high - middle, 0.0)),
    )


def gates(team, input_gate, forget_gate):
    first = team == 0
    given = jnp.where(first, input_gate[0:1, :], input_gate[1:2, :])
    forget = jnp.where(first, forget_gate[0:1, :], forget_gate[1:2, :])
    small = jnp.exp(-jnp.abs(forget))
    tail = jnp.where(small < 1e-4, small - 0.5 * small * small, jnp.log(1.0 + small))
    log_forget = jnp.minimum(forget, 0.0) - tail
    upto = jnp.where(iota((BLOCK, BLOCK), 0) <= iota((BLOCK, BLOCK), 1), 1.0, 0.0)
    cumulative = jnp.dot(
        jnp.broadcast_to(log_forget, (8, BLOCK)), upto, preferred_element_type=f32, precision=HIGHEST
    )[0:1, :]
    return given, cumulative


def pack_kernel(gate, up, down, packed, sem):
    copies = [
        pltpu.make_async_copy(gate, packed.at[0:D, :], sem.at[0]),
        pltpu.make_async_copy(up, packed.at[D : 2 * D, :], sem.at[1]),
    ]
    for k in range(16):
        copies.append(
            pltpu.make_async_copy(
                down.at[:, 128 * k : 128 * (k + 1)],
                packed.at[2 * D + 128 * k : 2 * D + 128 * (k + 1), :],
                sem.at[2 + k],
            )
        )
    for copy in copies:
        copy.start()
    for copy in copies:
        copy.wait()


def normalize(x, gain):
    rows = x[...].astype(f32)
    scale = lax.rsqrt(jnp.mean(rows * rows, axis=-1, keepdims=True) + epsilon)
    return (rows * scale * gain[...]).astype(bf16)


def route_kernel(
    x, gain, ids, weights, keys, values, input_gate, forget_gate,
    send, w_high, w_low, staged, states, sem,
):
    y, core = lax.axis_index("y"), lax.axis_index("c")
    team, part = y // 4, lax.rem(y, 2) * 2 + core
    normal = normalize(x, gain)
    expert = iota((N_EP, TOKENS), 0) * 2 + team
    named = jnp.zeros((N_EP, TOKENS), f32)
    weight = jnp.zeros((N_EP, TOKENS), f32)
    for k in range(4):
        hit = ids[k : k + 1, :] == expert
        named = named + jnp.where(hit, 1.0, 0.0)
        weight = weight + jnp.where(hit, weights[k : k + 1, :], 0.0)
    before = jnp.where(iota((TOKENS, TOKENS), 0) < iota((TOKENS, TOKENS), 1), 1.0, 0.0).astype(bf16)
    rank = jnp.dot(named.astype(bf16), before, preferred_element_type=f32)
    rank = jnp.where(named > 0.0, rank, -1.0)
    spread = jnp.where(iota((ROWS, N_EP), 0) // SLOTS == iota((ROWS, N_EP), 1), 1.0, 0.0)
    rank = jnp.dot(spread.astype(bf16), rank.astype(bf16), preferred_element_type=f32)
    weight = jnp.dot(spread, weight, preferred_element_type=f32, precision=HIGHEST)
    slot = (lax.rem(iota((ROWS, TOKENS), 0), SLOTS) + part * SLOTS).astype(f32)
    chosen = rank == slot
    pick = jnp.where(chosen, 1.0, 0.0).astype(bf16)
    copies = []
    for k in range(4):
        at = slice(512 * k, 512 * (k + 1))
        staged[:, at] = jnp.dot(pick, normal[:, at], preferred_element_type=f32).astype(bf16)
        copies.append(pltpu.make_async_copy(staged.at[:, at], send.at[:, at], sem.at[k]))
        copies[-1].start()
    weight = jnp.where(chosen, weight, 0.0)
    high = weight.astype(bf16)
    w_high[...] = high
    w_low[...] = (weight - high.astype(f32)).astype(bf16)

    given, cumulative = gates(team, input_gate, forget_gate)
    block_total = cumulative[:, BLOCK - 1 : BLOCK]
    log_keep = block_total - cumulative + given
    running = jnp.max(log_keep, axis=1, keepdims=True)
    kept = jnp.exp(log_keep - running)
    key = keys[:, pl.ds(pl.multiple_of(team * KEY_DIM, KEY_DIM), KEY_DIM)].astype(f32)
    memory = jnp.dot(
        values[...].astype(f32) * kept, key, preferred_element_type=f32, precision=HIGHEST
    )
    normalizer = jnp.dot(
        jnp.broadcast_to(kept, (8, BLOCK)), key, preferred_element_type=f32, precision=HIGHEST
    )
    states[:, 0, :] = memory[0:32, 0:128]
    states[:, 1, :] = memory[0:32, 128:256]
    states[:, 2, :] = memory[32:64, 0:128]
    states[:, 3, :] = memory[32:64, 128:256]
    states[:, 4, :] = jnp.broadcast_to(normalizer[0:1, 0:128], (N_EP, 128))
    states[:, 5, :] = jnp.broadcast_to(normalizer[0:1, 128:256], (N_EP, 128))
    states[:, 6, :] = split_scalar(block_total)
    states[:, 7, :] = split_scalar(running)
    staged[:, D:WIDE] = states[...].reshape(ROWS, 128).astype(bf16)
    copies.append(pltpu.make_async_copy(staged.at[:, D:WIDE], send.at[:, D:WIDE], sem.at[4]))
    copies[-1].start()
    for copy in copies:
        copy.wait()


def as_row(column):
    return jnp.broadcast_to(
        jnp.broadcast_to(column, (N_EP, 128))[None], (4, N_EP, 128)
    ).reshape(128, 128).T[0:N_EP, 0:N_EP]


def prefix(states):
    totals = as_row(jnp.sum(states[:, 6, :], axis=1, keepdims=True))
    peaks = as_row(jnp.sum(states[:, 7, :], axis=1, keepdims=True))
    row, column = iota((N_EP, N_EP), 0), iota((N_EP, N_EP), 1)
    earlier = column < row
    passed = jnp.where(earlier, totals, 0.0)
    later = jnp.where(row > column, 1.0, 0.0)
    between = jnp.dot(passed, later, preferred_element_type=f32, precision=HIGHEST)
    reach = jnp.where(earlier, peaks + between, lowest)
    running = jnp.maximum(
        jnp.sum(passed, axis=1, keepdims=True), jnp.max(reach, axis=1, keepdims=True)
    )
    share = jnp.where(earlier, jnp.exp(reach - running), 0.0)
    for k in range(6):
        states[:, k, :] = jnp.dot(
            share, states[:, k, :], preferred_element_type=f32, precision=HIGHEST
        )
    states[:, 6, :] = split_scalar(running)
    states[:, 7, :] = jnp.zeros((N_EP, 128), f32)


def expert_kernel(x, own, beside, near, far, out, staged, states, taken, sem, fetch):
    fetches = [
        pltpu.make_async_copy(pack, taken.at[k], fetch.at[k])
        for k, pack in enumerate((beside, near, far))
    ]
    for copy in fetches:
        copy.start()
    states[...] = x[:, D:WIDE].astype(f32).reshape(N_EP, 8, 128)
    prefix(states)
    staged[:, D:WIDE] = states[...].reshape(ROWS, 128).astype(bf16)
    copies = [pltpu.make_async_copy(staged.at[:, D:WIDE], out.at[:, D:WIDE], sem.at[0])]
    copies[0].start()
    rows = x[:, 0:D]
    packs = (own, taken.at[0], taken.at[1], taken.at[2])
    acts = []
    for k, pack in enumerate(packs):
        if k > 0:
            fetches[k - 1].wait()
        both = jnp.dot(
            rows,
            jnp.concatenate([pack[0:D, :], pack[D : 2 * D, :]], axis=1),
            preferred_element_type=f32,
        )
        gate, up = both[:, 0:128], both[:, 128:256]
        acts.append((gate / (1.0 + jnp.exp(-gate)) * up).astype(bf16))
    act = jnp.concatenate(acts, axis=1)
    for k in range(8):
        low = 2 * D + 256 * k
        down = jnp.concatenate(
            [
                jnp.concatenate(
                    [pack[low : low + 128, :], pack[low + 128 : low + 256, :]], axis=1
                )
                for pack in packs
            ],
            axis=0,
        )
        at = slice(256 * k, 256 * (k + 1))
        staged[:, at] = jnp.dot(act, down, preferred_element_type=f32).astype(bf16)
        copies.append(pltpu.make_async_copy(staged.at[:, at], out.at[:, at], sem.at[k + 1]))
        copies[-1].start()
    for copy in copies:
        copy.wait()


def shared_kernel(x, gain, gate, up, act):
    rows = normalize(x, gain)
    gated = lax.dot_general(rows, gate[...], NT, preferred_element_type=f32)
    lifted = lax.dot_general(rows, up[...], NT, preferred_element_type=f32)
    act[...] = (gated / (1.0 + jnp.exp(-gated)) * lifted).astype(bf16)


def combine_kernel(
    back, w_high, w_low, act, down, queries, keys, values, out_gate, input_gate, forget_gate, mix,
    keep, give, states, mixed, total,
):
    core = lax.axis_index("c")
    team = lax.axis_index("y") // 4
    states[...] = back[:, D:WIDE].astype(f32).reshape(N_EP, 8, 128)
    given, cumulative = gates(team, input_gate, forget_gate)
    at = pl.ds(pl.multiple_of(team * KEY_DIM, KEY_DIM), KEY_DIM)
    query, key = queries[:, at], keys[:, at]
    factor = KEY_DIM ** (-0.5)
    carried = cumulative + jnp.sum(states[0, 6:7, :], axis=1, keepdims=True)
    source = jnp.broadcast_to(given - cumulative, (BLOCK, BLOCK)).T
    allowed = iota((BLOCK, BLOCK), 0) <= iota((BLOCK, BLOCK), 1)
    log_weight = jnp.where(allowed, cumulative + source, lowest)
    stabilizer = jnp.maximum(carried, jnp.max(log_weight, axis=0, keepdims=True))
    within = jnp.exp(log_weight - stabilizer)
    across = jnp.exp(carried - stabilizer)
    scores = lax.dot_general(key, query, NT, preferred_element_type=f32) * factor
    weights = scores * within
    scaled = (query.astype(f32) * factor).astype(bf16)

    def read(first, second):
        return lax.dot_general(
            first.astype(bf16), scaled[:, 0:128], NT, preferred_element_type=f32
        ) + lax.dot_general(second.astype(bf16), scaled[:, 128:256], NT, preferred_element_type=f32)

    numerator = jnp.concatenate(
        [read(states[:, 0, :], states[:, 1, :]), read(states[:, 2, :], states[:, 3, :])], axis=0
    )
    numerator = across * numerator + jnp.dot(
        values[...], weights.astype(bf16), preferred_element_type=f32
    )
    normalizer = read(
        jnp.broadcast_to(states[0, 4:5, :], (16, 128)),
        jnp.broadcast_to(states[0, 5:6, :], (16, 128)),
    )
    denominator = across * normalizer[0:1, :] + jnp.sum(weights, axis=0, keepdims=True)
    hidden = numerator / jnp.maximum(jnp.abs(denominator), den_floor)
    gated = (hidden / (1.0 + jnp.exp(-out_gate[...].astype(f32)))).astype(bf16)
    mixed[...] = lax.dot_general(gated, mix[...], TN, preferred_element_type=f32)
    rows = back[:, 0:D]
    total[...] = (
        lax.dot_general(w_high[...], rows, TN, preferred_element_type=f32)
        + lax.dot_general(w_low[...], rows, TN, preferred_element_type=f32)
        + jnp.dot(act[...], down[...], preferred_element_type=f32)
    )
    for target, first in ((keep, core), (give, 1 - core)):
        for k in range(N_Y):
            start = pl.multiple_of(first * (TOKENS // 2) + k * E_ROWS, E_ROWS)
            target[k, 0:E_ROWS, :] = total[pl.ds(start, E_ROWS), :].astype(target.dtype)
            start = pl.multiple_of(first * (BLOCK // 2) + k * M_ROWS, M_ROWS)
            target[k, E_ROWS:PIECE, :] = mixed[pl.ds(start, M_ROWS), :].astype(target.dtype)


def place_kernel(mine, other, mixer, expert, sem):
    core = lax.axis_index("c")
    copies = []
    for half, (source, first) in enumerate(((mine, core), (other, 1 - core))):
        for k in range(N_Y):
            start = pl.multiple_of(first * (TOKENS // 2) + k * E_ROWS, E_ROWS)
            copies.append(
                pltpu.make_async_copy(
                    source.at[k, 0:E_ROWS, :], expert.at[pl.ds(start, E_ROWS), :], sem.at[half, k, 0]
                )
            )
            start = pl.multiple_of(first * (BLOCK // 2) + k * M_ROWS, M_ROWS)
            copies.append(
                pltpu.make_async_copy(
                    source.at[k, E_ROWS:PIECE, :], mixer.at[pl.ds(start, M_ROWS), :], sem.at[half, k, 1]
                )
            )
    for copy in copies:
        copy.start()
    for copy in copies:
        copy.wait()


def exchange(array, axis):
    return lax.all_to_all(array, axis, split_axis=0, concat_axis=0, tiled=True)


def swap(array):
    return lax.ppermute(array, "c", [(0, 1), (1, 0)])


def reach_over(array):
    return lax.ppermute(array, "y", [(k, k ^ 1) for k in range(N_Y)])


def after(array, *earlier):
    return lax.optimization_barrier((array, *earlier))[0]


def shards(
    queries,
    key_vectors,
    values,
    out_gate,
    input_gate,
    forget_gate,
    mix_weight,
    expert_input,
    norm_gain,
    route_ids,
    route_weights,
    expert_gate,
    expert_up,
    expert_down,
    shared_gate,
    shared_up,
    shared_down,
):
    dma = pltpu.SemaphoreType.DMA
    (own,) = call(
        pack_kernel,
        (expert_gate[0], expert_up[0], expert_down[0]),
        [HBM] * 3,
        [shape((3 * D, 128), bf16)],
        [VMEM],
        [dma((18,))],
        1 << 20,
    )
    near = reach_over(own)
    values_t, out_gate_t = values.T, out_gate.T
    input_t, forget_t = input_gate.T, forget_gate.T
    send, w_high, w_low = call(
        route_kernel,
        (
            expert_input,
            norm_gain[None, :],
            route_ids.T,
            route_weights.T,
            key_vectors,
            values_t,
            input_t,
            forget_t,
        ),
        [VMEM] * 8,
        [
            shape((ROWS, WIDE), bf16),
            shape((ROWS, TOKENS), bf16),
            shape((ROWS, TOKENS), bf16),
        ],
        [HBM] + [VMEM] * 2,
        [pltpu.VMEM((ROWS, WIDE), bf16), pltpu.VMEM((N_EP, 8, 128), f32), dma((5,))],
        1 << 28,
    )
    arrived = exchange(send.reshape(N_EP, SLOTS, WIDE), EP).reshape(ROWS, WIDE)
    beside = swap(after(own, w_high))
    far = swap(near)
    (act,) = call(
        shared_kernel,
        (after(expert_input, w_high), norm_gain[None, :], shared_gate.T, shared_up.T),
        [VMEM] * 4,
        [shape((TOKENS, 32), bf16)],
        [VMEM],
        [],
        1 << 26,
    )
    (results,) = call(
        expert_kernel,
        (arrived, own, beside, near, far),
        [VMEM] * 2 + [HBM] * 3,
        [shape((ROWS, WIDE), bf16)],
        [HBM],
        [
            pltpu.VMEM((ROWS, WIDE), bf16),
            pltpu.VMEM((N_EP, 8, 128), f32),
            pltpu.VMEM((3, 3 * D, 128), bf16),
            dma((9,)),
            dma((3,)),
        ],
        1 << 31,
        24,
    )
    back = exchange(results.reshape(N_EP, SLOTS, WIDE), EP).reshape(ROWS, WIDE)
    keep, give = call(
        combine_kernel,
        (
            back,
            w_high,
            w_low,
            act,
            shared_down,
            queries,
            key_vectors,
            values_t,
            out_gate_t,
            input_t,
            forget_t,
            mix_weight,
        ),
        [VMEM] * 12,
        [shape((N_Y, PIECE, D), f32), shape((N_Y, PIECE, D), bf16)],
        [VMEM] * 2,
        [
            pltpu.VMEM((N_EP, 8, 128), f32),
            pltpu.VMEM((BLOCK, D), f32),
            pltpu.VMEM((TOKENS, D), f32),
        ],
        1 << 28,
    )
    half = (keep + swap(give).astype(f32)).astype(bf16)
    piece = exchange(half, "y").astype(f32).sum(axis=0).astype(bf16)
    mine = exchange(jnp.broadcast_to(piece[None], (N_Y, PIECE, D)), "y")
    other = swap(mine)
    return call(
        place_kernel,
        (mine, other),
        [VMEM] * 2,
        [shape((BLOCK, D), bf16), shape((TOKENS, D), bf16)],
        [HBM] * 2,
        [dma((2, N_Y, 2))],
        1 << 20,
    )


def solution(mesh):
    finer = Mesh(mesh.devices.reshape(8, 4, N_Y, 2), EP_TP)
    placed = (
        P(EP, None),
        P(EP, None),
        P(EP, TP),
        P(EP, TP),
        P(EP, None),
        P(EP, None),
        P(TP, None),
        P(EP, None),
        P(),
        P(EP, None),
        P(EP, None),
        P(EP_TP, None, None),
        P(EP_TP, None, None),
        P(EP_TP, None, None),
        P(None, TP),
        P(None, TP),
        P(TP, None),
    )
    return jax.shard_map(
        shards, mesh=finer, in_specs=placed, out_specs=(P(EP, None), P(EP, None)), check_vma=False
    )
```

```python
import jax
import jax.numpy as jnp
from jax import lax
from jax.experimental import pallas as pl
from jax.experimental.pallas import tpu as pltpu
from jax.sharding import Mesh
from jax.sharding import PartitionSpec as P

D = 2048
WIDE = D + 128
KEY_DIM = 256
BLOCK = 128
N_EP = 32
N_Y = 8
SLOTS = 8
TOKENS = 256
ROWS = N_EP * SLOTS
E_ROWS = TOKENS // 16
M_ROWS = BLOCK // 16
PIECE = E_ROWS + M_ROWS
EP = ("z", "x")
WHOLE = 67_000_000
EP_TP = ("z", "x", "y", "c")
TP = ("y", "c")
bf16 = jnp.bfloat16
f32 = jnp.float32
epsilon = 1e-06
lowest = -1e30
den_floor = 4.0
HIGHEST = lax.Precision.HIGHEST

VMEM = pl.BlockSpec(memory_space=pltpu.VMEM)
HBM = pl.BlockSpec(memory_space=pltpu.HBM)
NT = (((1,), (1,)), ((), ()))
TN = (((0,), (0,)), ((), ()))


def call(body, arrays, ins, outs, spaces, scratch, flops, limit=16 << 20):
    return pl.pallas_call(
        body,
        out_shape=outs,
        in_specs=ins,
        out_specs=spaces,
        scratch_shapes=scratch,
        compiler_params=pltpu.CompilerParams(vmem_limit_bytes=limit),
        cost_estimate=pl.CostEstimate(flops=flops, bytes_accessed=1 << 20, transcendentals=0),
    )(*arrays)


def shape(dims, dtype):
    return jax.ShapeDtypeStruct(dims, dtype)


def iota(dims, dim):
    return lax.broadcasted_iota(jnp.int32, dims, dim)


def split_scalar(value):
    high = value.astype(bf16).astype(f32)
    middle = (value - high).astype(bf16).astype(f32)
    lane = iota((N_EP, 128), 1)
    return jnp.where(
        lane == 0,
        high,
        jnp.where(lane == 1, middle, jnp.where(lane == 2, value - high - middle, 0.0)),
    )


def gates(team, input_gate, forget_gate):
    first = team == 0
    given = jnp.where(first, input_gate[0:1, :], input_gate[1:2, :])
    forget = jnp.where(first, forget_gate[0:1, :], forget_gate[1:2, :])
    small = jnp.exp(-jnp.abs(forget))
    tail = jnp.where(small < 1e-4, small - 0.5 * small * small, jnp.log(1.0 + small))
    log_forget = jnp.minimum(forget, 0.0) - tail
    upto = jnp.where(iota((BLOCK, BLOCK), 0) <= iota((BLOCK, BLOCK), 1), 1.0, 0.0)
    cumulative = jnp.dot(
        jnp.broadcast_to(log_forget, (8, BLOCK)), upto, preferred_element_type=f32, precision=HIGHEST
    )[0:1, :]
    return given, cumulative


def normalize(x, gain):
    rows = x[...].astype(f32)
    scale = lax.rsqrt(jnp.mean(rows * rows, axis=-1, keepdims=True) + epsilon)
    return (rows * scale * gain[...]).astype(bf16)


def route_kernel(
    x, gain, ids, weights, keys, values, input_gate, forget_gate,
    send, w_high, w_low, staged, states, sem,
):
    y, core = lax.axis_index("y"), lax.axis_index("c")
    team, part = y // 4, lax.rem(y, 2) * 2 + core
    normal = normalize(x, gain)
    expert = iota((N_EP, TOKENS), 0) * 2 + team
    named = jnp.zeros((N_EP, TOKENS), f32)
    weight = jnp.zeros((N_EP, TOKENS), f32)
    for k in range(4):
        hit = ids[k : k + 1, :] == expert
        named = named + jnp.where(hit, 1.0, 0.0)
        weight = weight + jnp.where(hit, weights[k : k + 1, :], 0.0)
    before = jnp.where(iota((TOKENS, TOKENS), 0) < iota((TOKENS, TOKENS), 1), 1.0, 0.0).astype(bf16)
    rank = jnp.dot(named.astype(bf16), before, preferred_element_type=f32)
    rank = jnp.where(named > 0.0, rank, -1.0)
    spread = jnp.where(iota((ROWS, N_EP), 0) // SLOTS == iota((ROWS, N_EP), 1), 1.0, 0.0)
    rank = jnp.dot(spread.astype(bf16), rank.astype(bf16), preferred_element_type=f32)
    weight = jnp.dot(spread, weight, preferred_element_type=f32, precision=HIGHEST)
    slot = (lax.rem(iota((ROWS, TOKENS), 0), SLOTS) + part * SLOTS).astype(f32)
    chosen = rank == slot
    pick = jnp.where(chosen, 1.0, 0.0).astype(bf16)
    copies = []
    for k in range(4):
        at = slice(512 * k, 512 * (k + 1))
        staged[:, at] = jnp.dot(pick, normal[:, at], preferred_element_type=f32).astype(bf16)
        copies.append(pltpu.make_async_copy(staged.at[:, at], send.at[:, at], sem.at[k]))
        copies[-1].start()
    weight = jnp.where(chosen, weight, 0.0)
    high = weight.astype(bf16)
    w_high[...] = high
    w_low[...] = (weight - high.astype(f32)).astype(bf16)

    given, cumulative = gates(team, input_gate, forget_gate)
    block_total = cumulative[:, BLOCK - 1 : BLOCK]
    log_keep = block_total - cumulative + given
    running = jnp.max(log_keep, axis=1, keepdims=True)
    kept = jnp.exp(log_keep - running)
    key = keys[:, pl.ds(pl.multiple_of(team * KEY_DIM, KEY_DIM), KEY_DIM)].astype(f32)
    memory = jnp.dot(
        values[...].astype(f32) * kept, key, preferred_element_type=f32, precision=HIGHEST
    )
    normalizer = jnp.dot(
        jnp.broadcast_to(kept, (8, BLOCK)), key, preferred_element_type=f32, precision=HIGHEST
    )
    states[:, 0, :] = memory[0:32, 0:128]
    states[:, 1, :] = memory[0:32, 128:256]
    states[:, 2, :] = memory[32:64, 0:128]
    states[:, 3, :] = memory[32:64, 128:256]
    states[:, 4, :] = jnp.broadcast_to(normalizer[0:1, 0:128], (N_EP, 128))
    states[:, 5, :] = jnp.broadcast_to(normalizer[0:1, 128:256], (N_EP, 128))
    states[:, 6, :] = split_scalar(block_total)
    states[:, 7, :] = split_scalar(running)
    staged[:, D:WIDE] = states[...].reshape(ROWS, 128).astype(bf16)
    copies.append(pltpu.make_async_copy(staged.at[:, D:WIDE], send.at[:, D:WIDE], sem.at[4]))
    copies[-1].start()
    for copy in copies:
        copy.wait()


def as_row(column):
    return jnp.broadcast_to(
        jnp.broadcast_to(column, (N_EP, 128))[None], (4, N_EP, 128)
    ).reshape(128, 128).T[0:N_EP, 0:N_EP]


def prefix(states):
    totals = as_row(jnp.sum(states[:, 6, :], axis=1, keepdims=True))
    peaks = as_row(jnp.sum(states[:, 7, :], axis=1, keepdims=True))
    row, column = iota((N_EP, N_EP), 0), iota((N_EP, N_EP), 1)
    earlier = column < row
    passed = jnp.where(earlier, totals, 0.0)
    later = jnp.where(row > column, 1.0, 0.0)
    between = jnp.dot(passed, later, preferred_element_type=f32, precision=HIGHEST)
    reach = jnp.where(earlier, peaks + between, lowest)
    running = jnp.maximum(
        jnp.sum(passed, axis=1, keepdims=True), jnp.max(reach, axis=1, keepdims=True)
    )
    share = jnp.where(earlier, jnp.exp(reach - running), 0.0)
    for k in range(6):
        states[:, k, :] = jnp.dot(
            share, states[:, k, :], preferred_element_type=f32, precision=HIGHEST
        )
    states[:, 6, :] = split_scalar(running)
    states[:, 7, :] = jnp.zeros((N_EP, 128), f32)


def expert_kernel(*refs):
    x, weights = refs[0], refs[1:13]
    out, taken, wide, tall, staged, states, sem, fetch = refs[13:]
    first = pltpu.make_async_copy(x, taken, fetch.at[12])
    first.start()
    fetches = []
    for k in range(4):
        targets = (wide.at[k, :, 0:128], wide.at[k, :, 128:256], tall.at[128 * k : 128 * (k + 1), :])
        for j in range(3):
            fetches.append(pltpu.make_async_copy(weights[3 * k + j], targets[j], fetch.at[3 * k + j]))
            fetches[-1].start()
    first.wait()
    states[...] = taken[:, D:WIDE].astype(f32).reshape(N_EP, 8, 128)
    prefix(states)
    staged[:, D:WIDE] = states[...].reshape(ROWS, 128).astype(bf16)
    copies = [pltpu.make_async_copy(staged.at[:, D:WIDE], out.at[:, D:WIDE], sem.at[0])]
    copies[0].start()
    rows = taken[:, 0:D]
    acts = []
    for k in range(4):
        fetches[3 * k].wait()
        fetches[3 * k + 1].wait()
        both = jnp.dot(rows, wide[k], preferred_element_type=f32)
        gated, lifted = both[:, 0:128], both[:, 128:256]
        acts.append((gated / (1.0 + jnp.exp(-gated)) * lifted).astype(bf16))
    for k in range(4):
        fetches[3 * k + 2].wait()
    act = jnp.concatenate(acts, axis=1)
    for k in range(4):
        at = slice(512 * k, 512 * (k + 1))
        staged[:, at] = jnp.dot(act, tall[:, at], preferred_element_type=f32).astype(bf16)
        copies.append(pltpu.make_async_copy(staged.at[:, at], out.at[:, at], sem.at[k + 1]))
        copies[-1].start()
    for copy in copies:
        copy.wait()


def shared_kernel(x, gain, gate, up, act):
    rows = normalize(x, gain)
    gated = lax.dot_general(rows, gate[...], NT, preferred_element_type=f32)
    lifted = lax.dot_general(rows, up[...], NT, preferred_element_type=f32)
    act[...] = (gated / (1.0 + jnp.exp(-gated)) * lifted).astype(bf16)


def combine_kernel(
    back, w_high, w_low, act, down, queries, keys, values, out_gate, input_gate, forget_gate, mix,
    keep, give, states, mixed, total,
):
    core = lax.axis_index("c")
    team = lax.axis_index("y") // 4
    states[...] = back[:, D:WIDE].astype(f32).reshape(N_EP, 8, 128)
    given, cumulative = gates(team, input_gate, forget_gate)
    at = pl.ds(pl.multiple_of(team * KEY_DIM, KEY_DIM), KEY_DIM)
    query, key = queries[:, at], keys[:, at]
    factor = KEY_DIM ** (-0.5)
    carried = cumulative + jnp.sum(states[0, 6:7, :], axis=1, keepdims=True)
    source = jnp.broadcast_to(given - cumulative, (BLOCK, BLOCK)).T
    allowed = iota((BLOCK, BLOCK), 0) <= iota((BLOCK, BLOCK), 1)
    log_weight = jnp.where(allowed, cumulative + source, lowest)
    stabilizer = jnp.maximum(carried, jnp.max(log_weight, axis=0, keepdims=True))
    within = jnp.exp(log_weight - stabilizer)
    across = jnp.exp(carried - stabilizer)
    scores = lax.dot_general(key, query, NT, preferred_element_type=f32) * factor
    weights = scores * within
    scaled = (query.astype(f32) * factor).astype(bf16)

    def read(first, second):
        return lax.dot_general(
            first.astype(bf16), scaled[:, 0:128], NT, preferred_element_type=f32
        ) + lax.dot_general(second.astype(bf16), scaled[:, 128:256], NT, preferred_element_type=f32)

    numerator = jnp.concatenate(
        [read(states[:, 0, :], states[:, 1, :]), read(states[:, 2, :], states[:, 3, :])], axis=0
    )
    numerator = across * numerator + jnp.dot(
        values[...], weights.astype(bf16), preferred_element_type=f32
    )
    normalizer = read(
        jnp.broadcast_to(states[0, 4:5, :], (16, 128)),
        jnp.broadcast_to(states[0, 5:6, :], (16, 128)),
    )
    denominator = across * normalizer[0:1, :] + jnp.sum(weights, axis=0, keepdims=True)
    hidden = numerator / jnp.maximum(jnp.abs(denominator), den_floor)
    gated = (hidden / (1.0 + jnp.exp(-out_gate[...].astype(f32)))).astype(bf16)
    mixed[...] = lax.dot_general(gated, mix[...], TN, preferred_element_type=f32)
    rows = back[:, 0:D]
    total[...] = (
        lax.dot_general(w_high[...], rows, TN, preferred_element_type=f32)
        + lax.dot_general(w_low[...], rows, TN, preferred_element_type=f32)
        + jnp.dot(act[...], down[...], preferred_element_type=f32)
    )
    for target, first in ((keep, core), (give, 1 - core)):
        for k in range(N_Y):
            start = pl.multiple_of(first * (TOKENS // 2) + k * E_ROWS, E_ROWS)
            target[k, 0:E_ROWS, :] = total[pl.ds(start, E_ROWS), :].astype(target.dtype)
            start = pl.multiple_of(first * (BLOCK // 2) + k * M_ROWS, M_ROWS)
            target[k, E_ROWS:PIECE, :] = mixed[pl.ds(start, M_ROWS), :].astype(target.dtype)


def place_kernel(mine, other, mixer, expert, sem):
    core = lax.axis_index("c")
    copies = []
    for half, (source, first) in enumerate(((mine, core), (other, 1 - core))):
        for k in range(N_Y):
            start = pl.multiple_of(first * (TOKENS // 2) + k * E_ROWS, E_ROWS)
            copies.append(
                pltpu.make_async_copy(
                    source.at[k, 0:E_ROWS, :], expert.at[pl.ds(start, E_ROWS), :], sem.at[half, k, 0]
                )
            )
            start = pl.multiple_of(first * (BLOCK // 2) + k * M_ROWS, M_ROWS)
            copies.append(
                pltpu.make_async_copy(
                    source.at[k, E_ROWS:PIECE, :], mixer.at[pl.ds(start, M_ROWS), :], sem.at[half, k, 1]
                )
            )
    for copy in copies:
        copy.start()
    for copy in copies:
        copy.wait()


def exchange(array, axis):
    return lax.all_to_all(array, axis, split_axis=0, concat_axis=0, tiled=True)


def swap(array):
    return lax.ppermute(array, "c", [(0, 1), (1, 0)])


def reach_over(array):
    return lax.ppermute(array, "y", [(k, k ^ 1) for k in range(N_Y)])


def after(array, *earlier):
    return lax.optimization_barrier((array, *earlier))[0]


def shards(
    queries,
    key_vectors,
    values,
    out_gate,
    input_gate,
    forget_gate,
    mix_weight,
    expert_input,
    norm_gain,
    route_ids,
    route_weights,
    expert_gate,
    expert_up,
    expert_down,
    shared_gate,
    shared_up,
    shared_down,
):
    dma = pltpu.SemaphoreType.DMA
    own = (expert_gate[0], expert_up[0], expert_down[0])
    near_gate = reach_over(own[0])
    values_t, out_gate_t = values.T, out_gate.T
    input_t, forget_t = input_gate.T, forget_gate.T
    send, w_high, w_low = call(
        route_kernel,
        (
            expert_input,
            norm_gain[None, :],
            route_ids.T,
            route_weights.T,
            key_vectors,
            values_t,
            input_t,
            forget_t,
        ),
        [VMEM] * 8,
        [
            shape((ROWS, WIDE), bf16),
            shape((ROWS, TOKENS), bf16),
            shape((ROWS, TOKENS), bf16),
        ],
        [HBM] + [VMEM] * 2,
        [pltpu.VMEM((ROWS, WIDE), bf16), pltpu.VMEM((N_EP, 8, 128), f32), dma((5,))],
        1 << 28,
        WHOLE,
    )
    arrived = exchange(send.reshape(N_EP, SLOTS, WIDE), EP).reshape(ROWS, WIDE)
    near_up = reach_over(own[1])
    near_down = reach_over(after(own[2], w_high))
    near = (near_gate, near_up, near_down)
    beside = tuple(swap(after(array, w_high)) for array in own)
    far = tuple(swap(array) for array in near)
    (act,) = call(
        shared_kernel,
        (after(expert_input, w_high), norm_gain[None, :], shared_gate.T, shared_up.T),
        [VMEM] * 4,
        [shape((TOKENS, 32), bf16)],
        [VMEM],
        [],
        1 << 26,
    )
    (results,) = call(
        expert_kernel,
        (arrived,) + own + beside + near + far,
        [HBM] * 13,
        [shape((ROWS, WIDE), bf16)],
        [HBM],
        [
            pltpu.VMEM((ROWS, WIDE), bf16),
            pltpu.VMEM((4, D, 256), bf16),
            pltpu.VMEM((512, D), bf16),
            pltpu.VMEM((ROWS, WIDE), bf16),
            pltpu.VMEM((N_EP, 8, 128), f32),
            dma((5,)),
            dma((13,)),
        ],
        1 << 31,
        WHOLE,
    )
    back = exchange(results.reshape(N_EP, SLOTS, WIDE), EP).reshape(ROWS, WIDE)
    keep, give = call(
        combine_kernel,
        (
            back,
            w_high,
            w_low,
            act,
            shared_down,
            queries,
            key_vectors,
            values_t,
            out_gate_t,
            input_t,
            forget_t,
            mix_weight,
        ),
        [VMEM] * 12,
        [shape((N_Y, PIECE, D), f32), shape((N_Y, PIECE, D), bf16)],
        [VMEM] * 2,
        [
            pltpu.VMEM((N_EP, 8, 128), f32),
            pltpu.VMEM((BLOCK, D), f32),
            pltpu.VMEM((TOKENS, D), f32),
        ],
        1 << 28,
    )
    half = (keep + swap(give).astype(f32)).astype(bf16)
    piece = exchange(half, "y").astype(f32).sum(axis=0).astype(bf16)
    mine = exchange(jnp.broadcast_to(piece[None], (N_Y, PIECE, D)), "y")
    other = swap(mine)
    return call(
        place_kernel,
        (mine, other),
        [VMEM] * 2,
        [shape((BLOCK, D), bf16), shape((TOKENS, D), bf16)],
        [HBM] * 2,
        [dma((2, N_Y, 2))],
        1 << 20,
    )


def solution(mesh):
    finer = Mesh(mesh.devices.reshape(8, 4, N_Y, 2), EP_TP)
    placed = (
        P(EP, None),
        P(EP, None),
        P(EP, TP),
        P(EP, TP),
        P(EP, None),
        P(EP, None),
        P(TP, None),
        P(EP, None),
        P(),
        P(EP, None),
        P(EP, None),
        P(EP_TP, None, None),
        P(EP_TP, None, None),
        P(EP_TP, None, None),
        P(None, TP),
        P(None, TP),
        P(TP, None),
    )
    return jax.shard_map(
        shards, mesh=finer, in_specs=placed, out_specs=(P(EP, None), P(EP, None)), check_vma=False
    )
```

```python
import jax
import jax.numpy as jnp
from jax import lax
from jax.experimental import pallas as pl
from jax.experimental.pallas import tpu as pltpu
from jax.sharding import Mesh
from jax.sharding import PartitionSpec as P

D = 2048
WIDE = D + 128
KEY_DIM = 256
BLOCK = 128
N_EP = 32
N_Y = 8
SLOTS = 8
TOKENS = 256
ROWS = N_EP * SLOTS
E_ROWS = TOKENS // 16
M_ROWS = BLOCK // 16
PIECE = E_ROWS + M_ROWS
EP = ("z", "x")
WHOLE = 67_000_000
EP_TP = ("z", "x", "y", "c")
TP = ("y", "c")
bf16 = jnp.bfloat16
f32 = jnp.float32
epsilon = 1e-06
lowest = -1e30
den_floor = 4.0
HIGHEST = lax.Precision.HIGHEST

VMEM = pl.BlockSpec(memory_space=pltpu.VMEM)
HBM = pl.BlockSpec(memory_space=pltpu.HBM)
NT = (((1,), (1,)), ((), ()))
TN = (((0,), (0,)), ((), ()))


def call(body, arrays, ins, outs, spaces, scratch, flops, limit=16 << 20, aliases=None):
    return pl.pallas_call(
        body,
        out_shape=outs,
        in_specs=ins,
        out_specs=spaces,
        scratch_shapes=scratch,
        input_output_aliases=aliases or {},
        compiler_params=pltpu.CompilerParams(vmem_limit_bytes=limit),
        cost_estimate=pl.CostEstimate(flops=flops, bytes_accessed=1 << 20, transcendentals=0),
    )(*arrays)


def shape(dims, dtype):
    return jax.ShapeDtypeStruct(dims, dtype)


def iota(dims, dim):
    return lax.broadcasted_iota(jnp.int32, dims, dim)


def split_scalar(value):
    high = value.astype(bf16).astype(f32)
    middle = (value - high).astype(bf16).astype(f32)
    lane = iota((N_EP, 128), 1)
    return jnp.where(
        lane == 0,
        high,
        jnp.where(lane == 1, middle, jnp.where(lane == 2, value - high - middle, 0.0)),
    )


def gates(team, input_gate, forget_gate):
    first = team == 0
    given = jnp.where(first, input_gate[0:1, :], input_gate[1:2, :])
    forget = jnp.where(first, forget_gate[0:1, :], forget_gate[1:2, :])
    small = jnp.exp(-jnp.abs(forget))
    tail = jnp.where(small < 1e-4, small - 0.5 * small * small, jnp.log(1.0 + small))
    log_forget = jnp.minimum(forget, 0.0) - tail
    upto = jnp.where(iota((BLOCK, BLOCK), 0) <= iota((BLOCK, BLOCK), 1), 1.0, 0.0)
    cumulative = jnp.dot(
        jnp.broadcast_to(log_forget, (8, BLOCK)), upto, preferred_element_type=f32, precision=HIGHEST
    )[0:1, :]
    return given, cumulative


def normalize(x, gain):
    rows = x[...].astype(f32)
    scale = lax.rsqrt(jnp.mean(rows * rows, axis=-1, keepdims=True) + epsilon)
    return (rows * scale * gain[...]).astype(bf16)


def route_kernel(
    x, gain, ids, weights, keys, values, input_gate, forget_gate,
    send, w_high, w_low, staged, states, sem,
):
    y, core = lax.axis_index("y"), lax.axis_index("c")
    team, part = y // 4, lax.rem(y, 2) * 2 + core
    normal = normalize(x, gain)
    expert = iota((N_EP, TOKENS), 0) * 2 + team
    named = jnp.zeros((N_EP, TOKENS), f32)
    weight = jnp.zeros((N_EP, TOKENS), f32)
    for k in range(4):
        hit = ids[k : k + 1, :] == expert
        named = named + jnp.where(hit, 1.0, 0.0)
        weight = weight + jnp.where(hit, weights[k : k + 1, :], 0.0)
    before = jnp.where(iota((TOKENS, TOKENS), 0) < iota((TOKENS, TOKENS), 1), 1.0, 0.0).astype(bf16)
    rank = jnp.dot(named.astype(bf16), before, preferred_element_type=f32)
    rank = jnp.where(named > 0.0, rank, -1.0)
    spread = jnp.where(iota((ROWS, N_EP), 0) // SLOTS == iota((ROWS, N_EP), 1), 1.0, 0.0)
    rank = jnp.dot(spread.astype(bf16), rank.astype(bf16), preferred_element_type=f32)
    weight = jnp.dot(spread, weight, preferred_element_type=f32, precision=HIGHEST)
    slot = (lax.rem(iota((ROWS, TOKENS), 0), SLOTS) + part * SLOTS).astype(f32)
    chosen = rank == slot
    pick = jnp.where(chosen, 1.0, 0.0).astype(bf16)
    copies = []
    for k in range(4):
        at = slice(512 * k, 512 * (k + 1))
        staged[:, at] = jnp.dot(pick, normal[:, at], preferred_element_type=f32).astype(bf16)
        copies.append(pltpu.make_async_copy(staged.at[:, at], send.at[:, at], sem.at[k]))
        copies[-1].start()
    weight = jnp.where(chosen, weight, 0.0)
    high = weight.astype(bf16)
    w_high[...] = high
    w_low[...] = (weight - high.astype(f32)).astype(bf16)

    given, cumulative = gates(team, input_gate, forget_gate)
    block_total = cumulative[:, BLOCK - 1 : BLOCK]
    log_keep = block_total - cumulative + given
    running = jnp.max(log_keep, axis=1, keepdims=True)
    kept = jnp.exp(log_keep - running)
    key = keys[:, pl.ds(pl.multiple_of(team * KEY_DIM, KEY_DIM), KEY_DIM)].astype(f32)
    memory = jnp.dot(
        values[...].astype(f32) * kept, key, preferred_element_type=f32, precision=HIGHEST
    )
    normalizer = jnp.dot(
        jnp.broadcast_to(kept, (8, BLOCK)), key, preferred_element_type=f32, precision=HIGHEST
    )
    states[:, 0, :] = memory[0:32, 0:128]
    states[:, 1, :] = memory[0:32, 128:256]
    states[:, 2, :] = memory[32:64, 0:128]
    states[:, 3, :] = memory[32:64, 128:256]
    states[:, 4, :] = jnp.broadcast_to(normalizer[0:1, 0:128], (N_EP, 128))
    states[:, 5, :] = jnp.broadcast_to(normalizer[0:1, 128:256], (N_EP, 128))
    states[:, 6, :] = split_scalar(block_total)
    states[:, 7, :] = split_scalar(running)
    staged[:, D:WIDE] = states[...].reshape(ROWS, 128).astype(bf16)
    copies.append(pltpu.make_async_copy(staged.at[:, D:WIDE], send.at[:, D:WIDE], sem.at[4]))
    copies[-1].start()
    for copy in copies:
        copy.wait()


def as_row(column):
    return jnp.broadcast_to(
        jnp.broadcast_to(column, (N_EP, 128))[None], (4, N_EP, 128)
    ).reshape(128, 128).T[0:N_EP, 0:N_EP]


def prefix(states):
    totals = as_row(jnp.sum(states[:, 6, :], axis=1, keepdims=True))
    peaks = as_row(jnp.sum(states[:, 7, :], axis=1, keepdims=True))
    row, column = iota((N_EP, N_EP), 0), iota((N_EP, N_EP), 1)
    earlier = column < row
    passed = jnp.where(earlier, totals, 0.0)
    later = jnp.where(row > column, 1.0, 0.0)
    between = jnp.dot(passed, later, preferred_element_type=f32, precision=HIGHEST)
    reach = jnp.where(earlier, peaks + between, lowest)
    running = jnp.maximum(
        jnp.sum(passed, axis=1, keepdims=True), jnp.max(reach, axis=1, keepdims=True)
    )
    share = jnp.where(earlier, jnp.exp(reach - running), 0.0)
    for k in range(6):
        states[:, k, :] = jnp.dot(
            share, states[:, k, :], preferred_element_type=f32, precision=HIGHEST
        )
    states[:, 6, :] = split_scalar(running)
    states[:, 7, :] = jnp.zeros((N_EP, 128), f32)


def expert_kernel(*refs):
    x, weights = refs[0], refs[1:13]
    out, taken, wide, tall, staged, states, sem, fetch = refs[13:]
    first = pltpu.make_async_copy(x, taken, fetch.at[12])
    first.start()
    fetches = []
    for k in range(4):
        targets = (wide.at[k, :, 0:128], wide.at[k, :, 128:256], tall.at[128 * k : 128 * (k + 1), :])
        fetches.append(
            [
                pltpu.make_async_copy(weights[3 * k + j], targets[j], fetch.at[3 * k + j])
                for j in range(3)
            ]
        )
    for copy in fetches[0][0:2] + fetches[1][0:2]:
        copy.start()
    first.wait()
    for copy in fetches[2][0:2] + fetches[3][0:2]:
        copy.start()
    states[...] = taken[:, D:WIDE].astype(f32).reshape(N_EP, 8, 128)
    prefix(states)
    staged[:, D:WIDE] = states[...].reshape(ROWS, 128).astype(bf16)
    copies = [pltpu.make_async_copy(staged.at[:, D:WIDE], out.at[:, D:WIDE], sem.at[0])]
    copies[0].start()
    for k in range(4):
        fetches[k][2].start()
    rows = taken[:, 0:D]
    acts = []
    for k in range(4):
        fetches[k][0].wait()
        fetches[k][1].wait()
        both = jnp.dot(rows, wide[k], preferred_element_type=f32)
        gated, lifted = both[:, 0:128], both[:, 128:256]
        acts.append((gated / (1.0 + jnp.exp(-gated)) * lifted).astype(bf16))
    for k in range(4):
        fetches[k][2].wait()
    act = jnp.concatenate(acts, axis=1)
    for k in range(4):
        at = slice(512 * k, 512 * (k + 1))
        staged[:, at] = jnp.dot(act, tall[:, at], preferred_element_type=f32).astype(bf16)
        copies.append(pltpu.make_async_copy(staged.at[:, at], out.at[:, at], sem.at[k + 1]))
        copies[-1].start()
    for copy in copies:
        copy.wait()


def shared_kernel(x, gain, gate, up, act):
    rows = normalize(x, gain)
    gated = lax.dot_general(rows, gate[...], NT, preferred_element_type=f32)
    lifted = lax.dot_general(rows, up[...], NT, preferred_element_type=f32)
    act[...] = (gated / (1.0 + jnp.exp(-gated)) * lifted).astype(bf16)


def routed(back, w_high, w_low, act, down, half):
    at = pl.ds(pl.multiple_of(half * (TOKENS // 2), TOKENS // 2), TOKENS // 2)
    rows = back[:, 0:D]
    return (
        lax.dot_general(w_high[:, at], rows, TN, preferred_element_type=f32)
        + lax.dot_general(w_low[:, at], rows, TN, preferred_element_type=f32)
        + jnp.dot(act[at, :], down[...], preferred_element_type=f32)
    )


def give_kernel(
    back, w_high, w_low, act, down, queries, keys, values, out_gate, input_gate, forget_gate, mix,
    give, kept, states, mixed, total,
):
    core = lax.axis_index("c")
    team = lax.axis_index("y") // 4
    states[...] = back[:, D:WIDE].astype(f32).reshape(N_EP, 8, 128)
    given, cumulative = gates(team, input_gate, forget_gate)
    at = pl.ds(pl.multiple_of(team * KEY_DIM, KEY_DIM), KEY_DIM)
    query, key = queries[:, at], keys[:, at]
    factor = KEY_DIM ** (-0.5)
    carried = cumulative + jnp.sum(states[0, 6:7, :], axis=1, keepdims=True)
    source = jnp.broadcast_to(given - cumulative, (BLOCK, BLOCK)).T
    allowed = iota((BLOCK, BLOCK), 0) <= iota((BLOCK, BLOCK), 1)
    log_weight = jnp.where(allowed, cumulative + source, lowest)
    stabilizer = jnp.maximum(carried, jnp.max(log_weight, axis=0, keepdims=True))
    within = jnp.exp(log_weight - stabilizer)
    across = jnp.exp(carried - stabilizer)
    scores = lax.dot_general(key, query, NT, preferred_element_type=f32) * factor
    weights = scores * within
    scaled = (query.astype(f32) * factor).astype(bf16)

    def read(first, second):
        return lax.dot_general(
            first.astype(bf16), scaled[:, 0:128], NT, preferred_element_type=f32
        ) + lax.dot_general(second.astype(bf16), scaled[:, 128:256], NT, preferred_element_type=f32)

    numerator = jnp.concatenate(
        [read(states[:, 0, :], states[:, 1, :]), read(states[:, 2, :], states[:, 3, :])], axis=0
    )
    numerator = across * numerator + jnp.dot(
        values[...], weights.astype(bf16), preferred_element_type=f32
    )
    normalizer = read(
        jnp.broadcast_to(states[0, 4:5, :], (16, 128)),
        jnp.broadcast_to(states[0, 5:6, :], (16, 128)),
    )
    denominator = across * normalizer[0:1, :] + jnp.sum(weights, axis=0, keepdims=True)
    hidden = numerator / jnp.maximum(jnp.abs(denominator), den_floor)
    gated = (hidden / (1.0 + jnp.exp(-out_gate[...].astype(f32)))).astype(bf16)
    mixed[...] = lax.dot_general(gated, mix[...], TN, preferred_element_type=f32)
    total[...] = routed(back, w_high, w_low, act, down, 1 - core)
    for k in range(N_Y):
        give[k, 0:E_ROWS, :] = total[E_ROWS * k : E_ROWS * (k + 1), :].astype(bf16)
        start = pl.multiple_of((1 - core) * (BLOCK // 2) + k * M_ROWS, M_ROWS)
        give[k, E_ROWS:PIECE, :] = mixed[pl.ds(start, M_ROWS), :].astype(bf16)
    kept[...] = mixed[pl.ds(pl.multiple_of(core * (BLOCK // 2), BLOCK // 2), BLOCK // 2), :]


def keep_kernel(back, w_high, w_low, act, down, kept, keep, total):
    total[...] = routed(back, w_high, w_low, act, down, lax.axis_index("c"))
    for k in range(N_Y):
        keep[k, 0:E_ROWS, :] = total[E_ROWS * k : E_ROWS * (k + 1), :]
        keep[k, E_ROWS:PIECE, :] = kept[M_ROWS * k : M_ROWS * (k + 1), :]


def put(source, half, mixer, expert, sem):
    copies = []
    for k in range(N_Y):
        start = pl.multiple_of(half * (TOKENS // 2) + k * E_ROWS, E_ROWS)
        copies.append(
            pltpu.make_async_copy(
                source.at[k, 0:E_ROWS, :], expert.at[pl.ds(start, E_ROWS), :], sem.at[k, 0]
            )
        )
        start = pl.multiple_of(half * (BLOCK // 2) + k * M_ROWS, M_ROWS)
        copies.append(
            pltpu.make_async_copy(
                source.at[k, E_ROWS:PIECE, :], mixer.at[pl.ds(start, M_ROWS), :], sem.at[k, 1]
            )
        )
    for copy in copies:
        copy.start()
    for copy in copies:
        copy.wait()


def place_kernel(mine, mixer, expert, sem):
    put(mine, lax.axis_index("c"), mixer, expert, sem)


def fill_kernel(other, mixer_in, expert_in, mixer, expert, sem):
    put(other, 1 - lax.axis_index("c"), mixer, expert, sem)


def exchange(array, axis):
    return lax.all_to_all(array, axis, split_axis=0, concat_axis=0, tiled=True)


def swap(array):
    return lax.ppermute(array, "c", [(0, 1), (1, 0)])


def reach_over(array):
    return lax.ppermute(array, "y", [(k, k ^ 1) for k in range(N_Y)])


def after(array, *earlier):
    return lax.optimization_barrier((array, *earlier))[0]


def shards(
    queries,
    key_vectors,
    values,
    out_gate,
    input_gate,
    forget_gate,
    mix_weight,
    expert_input,
    norm_gain,
    route_ids,
    route_weights,
    expert_gate,
    expert_up,
    expert_down,
    shared_gate,
    shared_up,
    shared_down,
):
    dma = pltpu.SemaphoreType.DMA
    own = (expert_gate[0], expert_up[0], expert_down[0])
    near_gate = reach_over(own[0])
    values_t, out_gate_t = values.T, out_gate.T
    input_t, forget_t = input_gate.T, forget_gate.T
    send, w_high, w_low = call(
        route_kernel,
        (
            expert_input,
            norm_gain[None, :],
            route_ids.T,
            route_weights.T,
            key_vectors,
            values_t,
            input_t,
            forget_t,
        ),
        [VMEM] * 8,
        [
            shape((ROWS, WIDE), bf16),
            shape((ROWS, TOKENS), bf16),
            shape((ROWS, TOKENS), bf16),
        ],
        [HBM] + [VMEM] * 2,
        [pltpu.VMEM((ROWS, WIDE), bf16), pltpu.VMEM((N_EP, 8, 128), f32), dma((5,))],
        1 << 28,
        WHOLE,
    )
    arrived = exchange(send.reshape(N_EP, SLOTS, WIDE), EP).reshape(ROWS, WIDE)
    near_up = reach_over(after(own[1], w_high))
    near_down = reach_over(after(own[2], w_high))
    near = (near_gate, near_up, near_down)
    beside = tuple(swap(after(array, w_high)) for array in own)
    far = tuple(swap(array) for array in near)
    (act,) = call(
        shared_kernel,
        (after(expert_input, w_high), norm_gain[None, :], shared_gate.T, shared_up.T),
        [VMEM] * 4,
        [shape((TOKENS, 32), bf16)],
        [VMEM],
        [],
        1 << 26,
    )
    (results,) = call(
        expert_kernel,
        (arrived,) + own + beside + near + far,
        [HBM] * 13,
        [shape((ROWS, WIDE), bf16)],
        [HBM],
        [
            pltpu.VMEM((ROWS, WIDE), bf16),
            pltpu.VMEM((4, D, 256), bf16),
            pltpu.VMEM((512, D), bf16),
            pltpu.VMEM((ROWS, WIDE), bf16),
            pltpu.VMEM((N_EP, 8, 128), f32),
            dma((5,)),
            dma((13,)),
        ],
        1 << 31,
        WHOLE,
    )
    back = exchange(results.reshape(N_EP, SLOTS, WIDE), EP).reshape(ROWS, WIDE)
    give, kept = call(
        give_kernel,
        (
            back,
            w_high,
            w_low,
            act,
            shared_down,
            queries,
            key_vectors,
            values_t,
            out_gate_t,
            input_t,
            forget_t,
            mix_weight,
        ),
        [VMEM] * 12,
        [shape((N_Y, PIECE, D), bf16), shape((BLOCK // 2, D), f32)],
        [VMEM] * 2,
        [
            pltpu.VMEM((N_EP, 8, 128), f32),
            pltpu.VMEM((BLOCK, D), f32),
            pltpu.VMEM((TOKENS // 2, D), f32),
        ],
        1 << 28,
    )
    (keep,) = call(
        keep_kernel,
        (back, w_high, w_low, act, shared_down, kept),
        [VMEM] * 6,
        [shape((N_Y, PIECE, D), f32)],
        [VMEM],
        [pltpu.VMEM((TOKENS // 2, D), f32)],
        1 << 28,
    )
    half = (keep + swap(give).astype(f32)).astype(bf16)
    piece = exchange(half, "y").astype(f32).sum(axis=0).astype(bf16)
    mine = exchange(jnp.broadcast_to(piece[None], (N_Y, PIECE, D)), "y")
    other = swap(mine)
    outs = [shape((BLOCK, D), bf16), shape((TOKENS, D), bf16)]
    mixer, expert = call(
        place_kernel, (mine,), [VMEM], outs, [HBM] * 2, [dma((N_Y, 2))], 1 << 24
    )
    return call(
        fill_kernel,
        (other, mixer, expert),
        [VMEM] + [HBM] * 2,
        outs,
        [HBM] * 2,
        [dma((N_Y, 2))],
        1 << 24,
        aliases={1: 0, 2: 1},
    )


def solution(mesh):
    finer = Mesh(mesh.devices.reshape(8, 4, N_Y, 2), EP_TP)
    placed = (
        P(EP, None),
        P(EP, None),
        P(EP, TP),
        P(EP, TP),
        P(EP, None),
        P(EP, None),
        P(TP, None),
        P(EP, None),
        P(),
        P(EP, None),
        P(EP, None),
        P(EP_TP, None, None),
        P(EP_TP, None, None),
        P(EP_TP, None, None),
        P(None, TP),
        P(None, TP),
        P(TP, None),
    )
    return jax.shard_map(
        shards, mesh=finer, in_specs=placed, out_specs=(P(EP, None), P(EP, None)), check_vma=False
    )
```

```python
import jax
import jax.numpy as jnp
from jax import lax
from jax.experimental import pallas as pl
from jax.experimental.pallas import tpu as pltpu
from jax.sharding import Mesh
from jax.sharding import PartitionSpec as P

D = 2048
WIDE = D + 128
KEY_DIM = 256
BLOCK = 128
N_EP = 32
N_Y = 8
SLOTS = 8
TOKENS = 256
ROWS = N_EP * SLOTS
E_ROWS = TOKENS // 16
M_ROWS = BLOCK // 16
PIECE = E_ROWS + M_ROWS
EP = ("z", "x")
WHOLE = 67_000_000
EP_TP = ("z", "x", "y", "c")
TP = ("y", "c")
bf16 = jnp.bfloat16
f32 = jnp.float32
epsilon = 1e-06
lowest = -1e30
den_floor = 4.0

VMEM = pl.BlockSpec(memory_space=pltpu.VMEM)
HBM = pl.BlockSpec(memory_space=pltpu.HBM)
NT = (((1,), (1,)), ((), ()))
TN = (((0,), (0,)), ((), ()))


def call(body, arrays, ins, outs, spaces, scratch, flops, limit=16 << 20, aliases=None):
    return pl.pallas_call(
        body,
        out_shape=outs,
        in_specs=ins,
        out_specs=spaces,
        scratch_shapes=scratch,
        input_output_aliases=aliases or {},
        compiler_params=pltpu.CompilerParams(vmem_limit_bytes=limit),
        cost_estimate=pl.CostEstimate(flops=flops, bytes_accessed=1 << 20, transcendentals=0),
    )(*arrays)


def shape(dims, dtype):
    return jax.ShapeDtypeStruct(dims, dtype)


def iota(dims, dim):
    return lax.broadcasted_iota(jnp.int32, dims, dim)


def exact_dot(left, right, parts):
    total, rest = None, left
    for _ in range(parts):
        piece = rest.astype(bf16)
        product = jnp.dot(piece, right, preferred_element_type=f32)
        total = product if total is None else total + product
        rest = rest - piece.astype(f32)
    return total


def split_scalar(value):
    high = value.astype(bf16).astype(f32)
    middle = (value - high).astype(bf16).astype(f32)
    lane = iota((N_EP, 128), 1)
    return jnp.where(
        lane == 0,
        high,
        jnp.where(lane == 1, middle, jnp.where(lane == 2, value - high - middle, 0.0)),
    )


def gates(team, input_gate, forget_gate):
    first = team == 0
    given = jnp.where(first, input_gate[0:1, :], input_gate[1:2, :])
    forget = jnp.where(first, forget_gate[0:1, :], forget_gate[1:2, :])
    small = jnp.exp(-jnp.abs(forget))
    tail = jnp.where(small < 1e-4, small - 0.5 * small * small, jnp.log(1.0 + small))
    log_forget = jnp.minimum(forget, 0.0) - tail
    upto = jnp.where(iota((BLOCK, BLOCK), 0) <= iota((BLOCK, BLOCK), 1), 1.0, 0.0)
    cumulative = exact_dot(jnp.broadcast_to(log_forget, (16, BLOCK)), upto.astype(bf16), 3)[0:1, :]
    return given, cumulative


def normalize(x, gain):
    rows = x[...].astype(f32)
    scale = lax.rsqrt(jnp.mean(rows * rows, axis=-1, keepdims=True) + epsilon)
    return (rows * scale * gain[...]).astype(bf16)


def route_kernel(
    x, gain, ids, weights, keys, values, input_gate, forget_gate,
    send, w_high, w_low, staged, states, sem,
):
    y, core = lax.axis_index("y"), lax.axis_index("c")
    team, part = y // 4, lax.rem(y, 2) * 2 + core
    normal = normalize(x, gain)
    expert = iota((N_EP, TOKENS), 0) * 2 + team
    named = jnp.zeros((N_EP, TOKENS), f32)
    weight = jnp.zeros((N_EP, TOKENS), f32)
    for k in range(4):
        hit = ids[k : k + 1, :] == expert
        named = named + jnp.where(hit, 1.0, 0.0)
        weight = weight + jnp.where(hit, weights[k : k + 1, :], 0.0)
    before = jnp.where(iota((TOKENS, TOKENS), 0) < iota((TOKENS, TOKENS), 1), 1.0, 0.0).astype(bf16)
    rank = jnp.dot(named.astype(bf16), before, preferred_element_type=f32)
    rank = jnp.where(named > 0.0, rank, -1.0)
    spread = jnp.where(iota((ROWS, N_EP), 0) // SLOTS == iota((ROWS, N_EP), 1), 1.0, 0.0)
    spread = spread.astype(bf16)
    rank = jnp.dot(spread, rank.astype(bf16), preferred_element_type=f32)
    upper = weight.astype(bf16)
    lower = (weight - upper.astype(f32)).astype(bf16)
    slot = (lax.rem(iota((ROWS, TOKENS), 0), SLOTS) + part * SLOTS).astype(f32)
    chosen = rank == slot
    pick = jnp.where(chosen, 1.0, 0.0).astype(bf16)
    copies = []
    for k in range(4):
        at = slice(512 * k, 512 * (k + 1))
        staged[:, at] = jnp.dot(pick, normal[:, at], preferred_element_type=f32).astype(bf16)
        copies.append(pltpu.make_async_copy(staged.at[:, at], send.at[:, at], sem.at[k]))
        copies[-1].start()
    for target, part_of in ((w_high, upper), (w_low, lower)):
        placed = jnp.dot(spread, part_of, preferred_element_type=f32)
        target[...] = jnp.where(chosen, placed, 0.0).astype(bf16)

    given, cumulative = gates(team, input_gate, forget_gate)
    block_total = cumulative[:, BLOCK - 1 : BLOCK]
    log_keep = block_total - cumulative + given
    running = jnp.max(log_keep, axis=1, keepdims=True)
    kept = jnp.exp(log_keep - running)
    key = keys[:, pl.ds(pl.multiple_of(team * KEY_DIM, KEY_DIM), KEY_DIM)]
    lifted = jnp.concatenate(
        [values[...].astype(f32) * kept, jnp.broadcast_to(kept, (16, BLOCK))], axis=0
    )
    memory = exact_dot(lifted, key, 2)
    normalizer = memory[64:65, :]
    states[:, 0, :] = memory[0:32, 0:128]
    states[:, 1, :] = memory[0:32, 128:256]
    states[:, 2, :] = memory[32:64, 0:128]
    states[:, 3, :] = memory[32:64, 128:256]
    states[:, 4, :] = jnp.broadcast_to(normalizer[0:1, 0:128], (N_EP, 128))
    states[:, 5, :] = jnp.broadcast_to(normalizer[0:1, 128:256], (N_EP, 128))
    states[:, 6, :] = split_scalar(block_total)
    states[:, 7, :] = split_scalar(running)
    staged[:, D:WIDE] = states[...].reshape(ROWS, 128).astype(bf16)
    copies.append(pltpu.make_async_copy(staged.at[:, D:WIDE], send.at[:, D:WIDE], sem.at[4]))
    copies[-1].start()
    for copy in copies:
        copy.wait()


def as_row(column):
    return jnp.broadcast_to(
        jnp.broadcast_to(column, (N_EP, 128))[None], (4, N_EP, 128)
    ).reshape(128, 128).T[0:N_EP, 0:N_EP]


def prefix(states):
    totals = as_row(jnp.sum(states[:, 6, :], axis=1, keepdims=True))
    peaks = as_row(jnp.sum(states[:, 7, :], axis=1, keepdims=True))
    row, column = iota((N_EP, N_EP), 0), iota((N_EP, N_EP), 1)
    earlier = column < row
    passed = jnp.where(earlier, totals, 0.0)
    later = jnp.where(row > column, 1.0, 0.0).astype(bf16)
    between = exact_dot(passed, later, 3)
    reach = jnp.where(earlier, peaks + between, lowest)
    running = jnp.maximum(
        jnp.sum(passed, axis=1, keepdims=True), jnp.max(reach, axis=1, keepdims=True)
    )
    share = jnp.where(earlier, jnp.exp(reach - running), 0.0)
    held = jnp.concatenate([states[:, k, :] for k in range(6)], axis=1).astype(bf16)
    entering = exact_dot(share, held, 2)
    for k in range(6):
        states[:, k, :] = entering[:, 128 * k : 128 * (k + 1)]
    states[:, 6, :] = split_scalar(running)
    states[:, 7, :] = jnp.zeros((N_EP, 128), f32)


def expert_kernel(*refs):
    x, weights = refs[0], refs[1:13]
    out, taken, wide, tall, staged, states, sem, fetch = refs[13:]
    first = pltpu.make_async_copy(x, taken, fetch.at[12])
    first.start()
    fetches = []
    for k in range(4):
        targets = (wide.at[k, :, 0:128], wide.at[k, :, 128:256], tall.at[128 * k : 128 * (k + 1), :])
        fetches.append(
            [
                pltpu.make_async_copy(weights[3 * k + j], targets[j], fetch.at[3 * k + j])
                for j in range(3)
            ]
        )
    for copy in fetches[0][0:2] + fetches[1][0:2]:
        copy.start()
    first.wait()
    for copy in fetches[2][0:2] + fetches[3][0:2]:
        copy.start()
    states[...] = taken[:, D:WIDE].astype(f32).reshape(N_EP, 8, 128)
    prefix(states)
    staged[:, D:WIDE] = states[...].reshape(ROWS, 128).astype(bf16)
    copies = [pltpu.make_async_copy(staged.at[:, D:WIDE], out.at[:, D:WIDE], sem.at[0])]
    copies[0].start()
    for k in range(4):
        fetches[k][2].start()
    rows = taken[:, 0:D]
    acts = []
    for k in range(4):
        fetches[k][0].wait()
        fetches[k][1].wait()
        both = jnp.dot(rows, wide[k], preferred_element_type=f32)
        gated, lifted = both[:, 0:128], both[:, 128:256]
        acts.append((gated / (1.0 + jnp.exp(-gated)) * lifted).astype(bf16))
    for k in range(4):
        fetches[k][2].wait()
    act = jnp.concatenate(acts, axis=1)
    for k in range(4):
        at = slice(512 * k, 512 * (k + 1))
        staged[:, at] = jnp.dot(act, tall[:, at], preferred_element_type=f32).astype(bf16)
        copies.append(pltpu.make_async_copy(staged.at[:, at], out.at[:, at], sem.at[k + 1]))
        copies[-1].start()
    for copy in copies:
        copy.wait()


def shared_kernel(x, gain, gate, up, act):
    rows = normalize(x, gain)
    gated = lax.dot_general(rows, gate[...], NT, preferred_element_type=f32)
    lifted = lax.dot_general(rows, up[...], NT, preferred_element_type=f32)
    act[...] = (gated / (1.0 + jnp.exp(-gated)) * lifted).astype(bf16)


def routed(back, w_high, w_low, act, down, half):
    at = pl.ds(pl.multiple_of(half * (TOKENS // 2), TOKENS // 2), TOKENS // 2)
    rows = back[:, 0:D]
    return (
        lax.dot_general(w_high[:, at], rows, TN, preferred_element_type=f32)
        + lax.dot_general(w_low[:, at], rows, TN, preferred_element_type=f32)
        + jnp.dot(act[at, :], down[...], preferred_element_type=f32)
    )


def give_kernel(
    back, w_high, w_low, act, down, queries, keys, values, out_gate, input_gate, forget_gate, mix,
    give, kept, states, mixed, total,
):
    core = lax.axis_index("c")
    team = lax.axis_index("y") // 4
    states[...] = back[:, D:WIDE].astype(f32).reshape(N_EP, 8, 128)
    given, cumulative = gates(team, input_gate, forget_gate)
    at = pl.ds(pl.multiple_of(team * KEY_DIM, KEY_DIM), KEY_DIM)
    query, key = queries[:, at], keys[:, at]
    factor = KEY_DIM ** (-0.5)
    carried = cumulative + jnp.sum(states[0, 6:7, :], axis=1, keepdims=True)
    source = jnp.broadcast_to(given - cumulative, (BLOCK, BLOCK)).T
    allowed = iota((BLOCK, BLOCK), 0) <= iota((BLOCK, BLOCK), 1)
    log_weight = jnp.where(allowed, cumulative + source, lowest)
    stabilizer = jnp.maximum(carried, jnp.max(log_weight, axis=0, keepdims=True))
    within = jnp.exp(log_weight - stabilizer)
    across = jnp.exp(carried - stabilizer)
    scores = lax.dot_general(key, query, NT, preferred_element_type=f32) * factor
    weights = scores * within
    scaled = (query.astype(f32) * factor).astype(bf16)

    def read(first, second):
        return lax.dot_general(
            first.astype(bf16), scaled[:, 0:128], NT, preferred_element_type=f32
        ) + lax.dot_general(second.astype(bf16), scaled[:, 128:256], NT, preferred_element_type=f32)

    numerator = jnp.concatenate(
        [read(states[:, 0, :], states[:, 1, :]), read(states[:, 2, :], states[:, 3, :])], axis=0
    )
    numerator = across * numerator + jnp.dot(
        values[...], weights.astype(bf16), preferred_element_type=f32
    )
    normalizer = read(
        jnp.broadcast_to(states[0, 4:5, :], (16, 128)),
        jnp.broadcast_to(states[0, 5:6, :], (16, 128)),
    )
    denominator = across * normalizer[0:1, :] + jnp.sum(weights, axis=0, keepdims=True)
    hidden = numerator / jnp.maximum(jnp.abs(denominator), den_floor)
    gated = (hidden / (1.0 + jnp.exp(-out_gate[...].astype(f32)))).astype(bf16)
    mixed[...] = lax.dot_general(gated, mix[...], TN, preferred_element_type=f32)
    total[...] = routed(back, w_high, w_low, act, down, 1 - core)
    for k in range(N_Y):
        give[k, 0:E_ROWS, :] = total[E_ROWS * k : E_ROWS * (k + 1), :].astype(bf16)
        start = pl.multiple_of((1 - core) * (BLOCK // 2) + k * M_ROWS, M_ROWS)
        give[k, E_ROWS:PIECE, :] = mixed[pl.ds(start, M_ROWS), :].astype(bf16)
    kept[...] = mixed[pl.ds(pl.multiple_of(core * (BLOCK // 2), BLOCK // 2), BLOCK // 2), :]


def keep_kernel(back, w_high, w_low, act, down, kept, keep, total):
    total[...] = routed(back, w_high, w_low, act, down, lax.axis_index("c"))
    for k in range(N_Y):
        keep[k, 0:E_ROWS, :] = total[E_ROWS * k : E_ROWS * (k + 1), :]
        keep[k, E_ROWS:PIECE, :] = kept[M_ROWS * k : M_ROWS * (k + 1), :]


def put(source, half, mixer, expert, sem):
    copies = []
    for k in range(N_Y):
        start = pl.multiple_of(half * (TOKENS // 2) + k * E_ROWS, E_ROWS)
        copies.append(
            pltpu.make_async_copy(
                source.at[k, 0:E_ROWS, :], expert.at[pl.ds(start, E_ROWS), :], sem.at[k, 0]
            )
        )
        start = pl.multiple_of(half * (BLOCK // 2) + k * M_ROWS, M_ROWS)
        copies.append(
            pltpu.make_async_copy(
                source.at[k, E_ROWS:PIECE, :], mixer.at[pl.ds(start, M_ROWS), :], sem.at[k, 1]
            )
        )
    for copy in copies:
        copy.start()
    for copy in copies:
        copy.wait()


def place_kernel(mine, mixer, expert, sem):
    put(mine, lax.axis_index("c"), mixer, expert, sem)


def fill_kernel(other, mixer_in, expert_in, mixer, expert, sem):
    put(other, 1 - lax.axis_index("c"), mixer, expert, sem)


def exchange(array, axis):
    return lax.all_to_all(array, axis, split_axis=0, concat_axis=0, tiled=True)


def swap(array):
    return lax.ppermute(array, "c", [(0, 1), (1, 0)])


def reach_over(array):
    return lax.ppermute(array, "y", [(k, k ^ 1) for k in range(N_Y)])


def after(array, *earlier):
    return lax.optimization_barrier((array, *earlier))[0]


def shards(
    queries,
    key_vectors,
    values,
    out_gate,
    input_gate,
    forget_gate,
    mix_weight,
    expert_input,
    norm_gain,
    route_ids,
    route_weights,
    expert_gate,
    expert_up,
    expert_down,
    shared_gate,
    shared_up,
    shared_down,
):
    dma = pltpu.SemaphoreType.DMA
    own = (expert_gate[0], expert_up[0], expert_down[0])
    near_gate = reach_over(own[0])
    values_t, out_gate_t = values.T, out_gate.T
    input_t, forget_t = input_gate.T, forget_gate.T
    send, w_high, w_low = call(
        route_kernel,
        (
            expert_input,
            norm_gain[None, :],
            route_ids.T,
            route_weights.T,
            key_vectors,
            values_t,
            input_t,
            forget_t,
        ),
        [VMEM] * 8,
        [
            shape((ROWS, WIDE), bf16),
            shape((ROWS, TOKENS), bf16),
            shape((ROWS, TOKENS), bf16),
        ],
        [HBM] + [VMEM] * 2,
        [pltpu.VMEM((ROWS, WIDE), bf16), pltpu.VMEM((N_EP, 8, 128), f32), dma((5,))],
        1 << 28,
        WHOLE,
    )
    arrived = exchange(send.reshape(N_EP, SLOTS, WIDE), EP).reshape(ROWS, WIDE)
    near_up = reach_over(after(own[1], w_high))
    near_down = reach_over(after(own[2], w_high))
    near = (near_gate, near_up, near_down)
    beside = tuple(swap(after(array, w_high)) for array in own)
    far = tuple(swap(array) for array in near)
    (act,) = call(
        shared_kernel,
        (after(expert_input, w_high), norm_gain[None, :], shared_gate.T, shared_up.T),
        [VMEM] * 4,
        [shape((TOKENS, 32), bf16)],
        [VMEM],
        [],
        1 << 26,
    )
    (results,) = call(
        expert_kernel,
        (arrived,) + own + beside + near + far,
        [HBM] * 13,
        [shape((ROWS, WIDE), bf16)],
        [HBM],
        [
            pltpu.VMEM((ROWS, WIDE), bf16),
            pltpu.VMEM((4, D, 256), bf16),
            pltpu.VMEM((512, D), bf16),
            pltpu.VMEM((ROWS, WIDE), bf16),
            pltpu.VMEM((N_EP, 8, 128), f32),
            dma((5,)),
            dma((13,)),
        ],
        1 << 31,
        WHOLE,
    )
    back = exchange(results.reshape(N_EP, SLOTS, WIDE), EP).reshape(ROWS, WIDE)
    give, kept = call(
        give_kernel,
        (
            back,
            w_high,
            w_low,
            act,
            shared_down,
            queries,
            key_vectors,
            values_t,
            out_gate_t,
            input_t,
            forget_t,
            mix_weight,
        ),
        [VMEM] * 12,
        [shape((N_Y, PIECE, D), bf16), shape((BLOCK // 2, D), f32)],
        [VMEM] * 2,
        [
            pltpu.VMEM((N_EP, 8, 128), f32),
            pltpu.VMEM((BLOCK, D), f32),
            pltpu.VMEM((TOKENS // 2, D), f32),
        ],
        1 << 28,
    )
    (keep,) = call(
        keep_kernel,
        (back, w_high, w_low, act, shared_down, kept),
        [VMEM] * 6,
        [shape((N_Y, PIECE, D), f32)],
        [VMEM],
        [pltpu.VMEM((TOKENS // 2, D), f32)],
        1 << 28,
    )
    half = (keep + swap(give).astype(f32)).astype(bf16)
    piece = exchange(half, "y").astype(f32).sum(axis=0).astype(bf16)
    mine = exchange(jnp.broadcast_to(piece[None], (N_Y, PIECE, D)), "y")
    other = swap(mine)
    outs = [shape((BLOCK, D), bf16), shape((TOKENS, D), bf16)]
    mixer, expert = call(
        place_kernel, (mine,), [VMEM], outs, [HBM] * 2, [dma((N_Y, 2))], 1 << 24
    )
    return call(
        fill_kernel,
        (other, mixer, expert),
        [VMEM] + [HBM] * 2,
        outs,
        [HBM] * 2,
        [dma((N_Y, 2))],
        1 << 24,
        aliases={1: 0, 2: 1},
    )


def solution(mesh):
    finer = Mesh(mesh.devices.reshape(8, 4, N_Y, 2), EP_TP)
    placed = (
        P(EP, None),
        P(EP, None),
        P(EP, TP),
        P(EP, TP),
        P(EP, None),
        P(EP, None),
        P(TP, None),
        P(EP, None),
        P(),
        P(EP, None),
        P(EP, None),
        P(EP_TP, None, None),
        P(EP_TP, None, None),
        P(EP_TP, None, None),
        P(None, TP),
        P(None, TP),
        P(TP, None),
    )
    return jax.shard_map(
        shards, mesh=finer, in_specs=placed, out_specs=(P(EP, None), P(EP, None)), check_vma=False
    )
```
